32 devices in a mesh: ep: 8 (over z, x), tp: 4 (over y, core).
Axes of the slice: x: 2, y: 2, z: 4, core: 2. Of those that a mesh axis runs over, the one named last changes fastest.
Arguments:
- tokens: bfloat16 [128, 2048], P('ep'), may hold values from -6 to 6
- norm1_gain: float32 [2048], replicated, may hold values from 0.1 to 1.9
- query_weight: bfloat16 [2048, 512], P(None, 'tp'), may hold values from -0.125 to 0.125
- key_weight: bfloat16 [2048, 256], P(None, 'tp'), may hold values from -0.125 to 0.125
- value_weight: bfloat16 [2048, 256], P(None, 'tp'), may hold values from -0.125 to 0.125
- forget_weight: bfloat16 [2048, 8], P(None, 'tp'), may hold values from -0.125 to 0.125
- forget_bias: float32 [8], P('tp'), may hold values from 0.5 to 4
- out_weight: bfloat16 [512, 2048], P('tp'), may hold values from -0.25 to 0.25
- kv_cache: bfloat16 [128, 1024, 4, 128], P('ep', None, 'tp'), may hold values from -6 to 6
- log_gates: float32 [128, 8, 1024], P('ep', 'tp'), may hold values from -1024 to 0, as said below
- lengths: int32 [128], P('ep'), may hold values from 64 to 1024
- norm2_gain: float32 [2048], replicated, may hold values from 0.1 to 1.9
- routing: int32 [128, 4], P('ep'), may hold values from 0 to 7, all different within a row; in each aligned block of 16 rows (0 to 15, 16 to 31, ...) at most 16 rows name the same one
- route_weight: float32 [128, 4], P('ep'), may hold values from 0.1 to 0.6
- expert_gate: bfloat16 [8, 2048, 2048], P('ep', None, 'tp'), may hold values from -0.25 to 0.25
- expert_up: bfloat16 [8, 2048, 2048], P('ep', None, 'tp'), may hold values from -0.25 to 0.25
- expert_down: bfloat16 [8, 2048, 2048], P('ep', 'tp'), may hold values from -0.0625 to 0.0625
- dense_gate: bfloat16 [2048, 4096], P(None, 'ep'), may hold values from -0.25 to 0.25
- dense_up: bfloat16 [2048, 4096], P(None, 'ep'), may hold values from -0.25 to 0.25
- dense_down: bfloat16 [4096, 2048], P('ep'), may hold values from -0.09375 to 0.09375
- dense_mix: float32 [2048], replicated, may hold values from -0.125 to 0.125
Outputs:
- layer_out: bfloat16 [128, 2048], P(('ep', 'tp'))
The draws below stay inside these ranges and needn't reach their ends.
Inputs may be any that keep to these rules, and one draw needn't show every extreme that they name: `log_gates`: Non-increasing along the positions. `routing`: each row names 4 different experts. Among the rows of one index of ep (aligned blocks of 16 rows) no expert is named by more than 16 rows, and in every draw some expert is named by exactly 16 rows of some block.
All inputs are finite; a program needn't handle non-finite values.
Results may differ from the reference program's by a relative error of at most 0.011.
Values may be sent and summed in bfloat16 or wider, within the bound.
No kernel may reach another device: no remote copies, remote signals or barrier semaphores. Data moves between devices by JAX's collectives and lax.ppermute only.
A program may use at most 128 MiB of HBM per device.

```python
import math
from functools import partial
import jax
import jax.numpy as jnp
import numpy as np
from jax import lax

D = 2048
QUERY_HEADS = 8
KV_HEADS = 4
HEAD_DIM = 64
EXP_FF = 2048
DENSE_FF = 4096
TOP = 4
SEQ_GRP = 16
CACHE_POSITIONS = 1024
BATCH_SEQUENCES = 128
EXPERTS = 8
CAP = 16
N_EP = 8


def draw_log_gates(key, part):
    random_subkeys = jax.random.split(jax.random.fold_in(key, 7), 6)
    slow_share = 0.5
    is_slow = jax.random.uniform(random_subkeys[0], (1, QUERY_HEADS, 1)) < slow_share
    slow_rate = jnp.exp(jax.random.uniform(random_subkeys[1], (1, QUERY_HEADS, 1), minval=jnp.log(0.3), maxval=jnp.log(1.5))) / CACHE_POSITIONS
    fast_rate = 1.0 / jnp.exp(jax.random.uniform(random_subkeys[2], (1, QUERY_HEADS, 1), minval=jnp.log(30.0), maxval=jnp.log(100.0)))
    per_seq = jnp.exp(jax.random.uniform(random_subkeys[3], (BATCH_SEQUENCES, 1, 1), minval=jnp.log(0.5), maxval=jnp.log(2.0)))
    roughness = jax.random.uniform(random_subkeys[4], (BATCH_SEQUENCES, QUERY_HEADS, CACHE_POSITIONS), minval=0.25, maxval=1.75)
    logarithm_increments = -jnp.where(is_slow, slow_rate, fast_rate) * per_seq * roughness
    spike_sample = jax.random.uniform(random_subkeys[5], (BATCH_SEQUENCES, QUERY_HEADS, CACHE_POSITIONS))
    spike_events = spike_sample < 3.0 / CACHE_POSITIONS
    spike_penalty = jnp.log(1.0 - (0.2 + 0.3 * jnp.clip(spike_sample * CACHE_POSITIONS / 3.0, 0.0, 1.0)))
    logarithm_increments = jnp.where(spike_events, logarithm_increments + spike_penalty, logarithm_increments)
    return jnp.cumsum(logarithm_increments, axis=2).astype(jnp.float32)


def touch_ends(entries, rng, low, largest):
    spot = [jax.random.randint(jax.random.fold_in(rng, axis), (), 0, length) for axis, length in enumerate(entries.shape)]
    widest = entries.shape.index(max(entries.shape))
    next_to = spot[:widest] + [(spot[widest] + 1) % entries.shape[widest]] + spot[widest + 1:]
    return entries.at[tuple(spot)].set(low).at[tuple(next_to)].set(largest)


def levels(key, extent, cuts, smallest, high):
    level = 1.0
    for axis_at, shards_of in cuts:
        heights = jax.random.uniform(jax.random.fold_in(jax.random.fold_in(key, 6), axis_at), (shards_of,), jnp.float32, smallest / len(cuts), high / len(cuts))
        level = level * jnp.repeat(jnp.exp(heights), extent[axis_at] // shards_of).reshape((-1,) + (1,) * (len(extent) - 1 - axis_at))
    return level


def shared_out(rng, own, number, rows, count, top, bound, lean):
    order = jax.random.permutation(rng, count)
    heavy_load, usual = portions_of(count, rows * top, bound, lean, True), portions_of(count, rows * top, bound, lean, False)
    places = jnp.arange(count)

    def named(tallies, offset_by):
        used = int((tallies > 0).sum())
        fixed = max(1, used // 4)
        shifted = fixed + (places - fixed + offset_by * (used - fixed)) % max(1, count - fixed)
        return jnp.zeros((count,), jnp.int32).at[order[jnp.where(places < fixed, places, shifted)]].set(jnp.asarray(tallies, jnp.int32))

    tallies = jnp.where(number % 4 == 0, named(heavy_load, number // 4), named(usual, number - number // 4 - 1))
    mixed = jax.random.permutation(jax.random.fold_in(own, 3), count)
    giver, receiver = mixed[0:count // 2 * 2:2], mixed[1:count // 2 * 2:2]
    slack = jnp.minimum(tallies[giver] - 1, bound - tallies[receiver]) // 2
    slack = jnp.where((giver == order[0]) | (receiver == order[0]) | (tallies[receiver] == 0), 0, jnp.maximum(slack, 0))
    shifted = jax.random.randint(jax.random.fold_in(own, 4), (count // 2,), 0, 1 << 20) % (slack + 1)
    tallies = tallies.at[giver].add(-shifted).at[receiver].add(shifted)
    members = jnp.searchsorted(jnp.cumsum(tallies), jnp.arange(rows * top), side="right").astype(jnp.int32)
    listing = members.reshape(top, rows).T
    listing = listing[jax.random.permutation(jax.random.fold_in(own, 1), rows)]
    offset_by = jax.random.randint(jax.random.fold_in(own, 2), (rows, 1), 0, top)
    return jnp.take_along_axis(listing, (jnp.arange(top)[None, :] + offset_by) % top, axis=1)


def portions_of(count, total, limit, lean, full):
    portions = [(1 << 20) // math.isqrt(rank ** lean) + 1 for rank in range(1, count + 1)]
    largest = limit if full else min(limit, max(-(-total // count), total * portions[0] // sum(portions)))
    least = 1 if total - largest >= count - 1 else 0
    holding, surplus = [largest] + [least] * (count - 1), total - largest - least * (count - 1)
    while surplus > 0:
        movable = [i for i in range(1, count) if holding[i] < largest] or [i for i in range(1, count) if holding[i] < limit]
        mass, left = sum([portions[i] for i in movable]), surplus
        for i in movable:
            more = min(limit - holding[i], max(1, left * portions[i] // mass), surplus)
            holding[i] = holding[i] + more
            surplus = surplus - more
    return np.array(holding)


def bell_draw(stream_key, extent, deviation, limit, cuts=(), kind=jnp.bfloat16):
    result = jax.random.normal(stream_key, extent, jnp.float32) * deviation
    if len(cuts) > 0:
        result = levels(stream_key, extent, cuts, -0.22, 0.18) * result
    return jnp.clip(result, min=-limit, max=limit).astype(kind)


def setup_inputs(seed: int = 0) -> dict:
    keys = jax.random.split(jax.random.key(seed), 22)
    tokens = bell_draw(keys[0], (BATCH_SEQUENCES, D), 1.0, 6.0, ((0, 8),))
    norm1_gain = jnp.clip(1.0 + 0.18 * jax.random.normal(keys[1], (D,), jnp.float32), 0.1, 1.9)
    query_weight = bell_draw(keys[2], (D, QUERY_HEADS * HEAD_DIM), D ** -0.5, 0.125, ((1, 4),))
    key_weight = bell_draw(keys[3], (D, KV_HEADS * HEAD_DIM), D ** -0.5, 0.125, ((1, 4),))
    value_weight = bell_draw(keys[4], (D, KV_HEADS * HEAD_DIM), D ** -0.5, 0.125, ((1, 4),))
    forget_weight = bell_draw(keys[5], (D, QUERY_HEADS), D ** -0.5, 0.125, ((1, 4),))
    forget_bias = jnp.clip(0.5 + 3.5 * jax.random.uniform(keys[6], (QUERY_HEADS,), jnp.float32) ** levels(keys[6], (QUERY_HEADS,), ((0, 4),), -0.2, 0.2), 0.5, 4.0)
    out_weight = bell_draw(keys[7], (QUERY_HEADS * HEAD_DIM, D), (QUERY_HEADS * HEAD_DIM) ** -0.5, 0.25, ((0, 4),))
    kv_cache = bell_draw(keys[8], (BATCH_SEQUENCES, CACHE_POSITIONS, KV_HEADS, 2 * HEAD_DIM), 1.0, 6.0, ((0, 8), (2, 4)))
    log_gates = draw_log_gates(jax.random.fold_in(keys[21], 71), 0)
    lengths = touch_ends(jax.random.randint(keys[10], (BATCH_SEQUENCES,), CACHE_POSITIONS // 16, CACHE_POSITIONS + 1), jax.random.fold_in(keys[10], 1), CACHE_POSITIONS // 16, CACHE_POSITIONS).astype(jnp.int32)
    norm2_gain = jnp.clip(1.0 + 0.18 * jax.random.normal(keys[11], (D,), jnp.float32), 0.1, 1.9)
    routing_keys = jax.random.split(jax.random.fold_in(keys[12], 1), BATCH_SEQUENCES // SEQ_GRP)
    routing_turns = jax.random.permutation(jax.random.fold_in(keys[12], 3), BATCH_SEQUENCES // SEQ_GRP)
    routing = jax.vmap(lambda own, number: shared_out(jax.random.fold_in(keys[12], 2), own, number, SEQ_GRP, EXPERTS, TOP, CAP, 2))(routing_keys, routing_turns).reshape((BATCH_SEQUENCES, TOP))
    route_weight = jnp.clip(0.1 + 0.5 * jax.random.uniform(keys[13], (BATCH_SEQUENCES, TOP), jnp.float32) ** levels(keys[13], (BATCH_SEQUENCES, TOP), ((0, 8),), -0.2, 0.2), 0.1, 0.6)
    expert_gate = bell_draw(keys[14], (EXPERTS, D, EXP_FF), (D // 4) ** -0.5, 0.25, ((0, 8), (2, 4)))
    expert_up = bell_draw(keys[15], (EXPERTS, D, EXP_FF), (D // 4) ** -0.5, 0.25, ((0, 8), (2, 4)))
    expert_down = bell_draw(keys[16], (EXPERTS, EXP_FF, D), (4 * EXP_FF) ** -0.5, 0.0625, ((0, 8), (1, 4)))
    dense_gate = bell_draw(keys[17], (D, DENSE_FF), (D // 4) ** -0.5, 0.25, ((1, 8),))
    dense_up = bell_draw(keys[18], (D, DENSE_FF), (D // 4) ** -0.5, 0.25, ((1, 8),))
    dense_down = bell_draw(keys[19], (DENSE_FF, D), DENSE_FF ** -0.5, 0.09375, ((0, 8),))
    dense_mix = bell_draw(keys[20], (D,), D ** -0.5, 0.125, (), jnp.float32)
    return dict(tokens=tokens, norm1_gain=norm1_gain, query_weight=query_weight, key_weight=key_weight, value_weight=value_weight, forget_weight=forget_weight, forget_bias=forget_bias, out_weight=out_weight, kv_cache=kv_cache, log_gates=log_gates, lengths=lengths, norm2_gain=norm2_gain, routing=routing, route_weight=route_weight, expert_gate=expert_gate, expert_up=expert_up, expert_down=expert_down, dense_gate=dense_gate, dense_up=dense_up, dense_down=dense_down, dense_mix=dense_mix)


EPS = 1e-05
LIMIT = 7.0
ALPHA = 1.702

def clamped_unit(gate_pre, up_pre):
    capped = jnp.minimum(gate_pre, LIMIT)
    return capped * jax.nn.sigmoid(ALPHA * capped) * (jnp.clip(up_pre, -LIMIT, LIMIT) + 1.0)

def rms_scaled(values, gain_vec):
    return values * lax.rsqrt(lax.optimization_barrier(jnp.mean(values * values, axis=-1, keepdims=True)) + EPS) * gain_vec

def slot_tables(routes, experts, capacity):
    flat_ids = routes.reshape(-1)
    onehot = (flat_ids[:, None] == jnp.arange(experts, dtype=jnp.int32)[None, :]).astype(jnp.int32)
    earlier = jnp.cumsum(onehot, axis=0, dtype=jnp.int32) - onehot
    slot_ids = lax.optimization_barrier(jnp.sum(earlier * onehot, axis=1, dtype=jnp.int32))
    matches = onehot[:, :, None] * (slot_ids[:, None, None] == jnp.arange(capacity, dtype=jnp.int32)[None, None, :]).astype(jnp.int32)
    owners = jnp.arange(flat_ids.shape[0], dtype=jnp.int32) // routes.shape[1]
    source = lax.optimization_barrier(jnp.sum(matches * owners[:, None, None], axis=0, dtype=jnp.int32))
    return (slot_ids, source)

def attend_group(block_args):
    queries, key_new, value_new, gate_new, cache, gates, seq_lens = block_args
    seq_count, cache_len, kv_heads, doubled = cache.shape
    head_dim = doubled // 2
    head_count = gate_new.shape[1]
    per_kv = head_count // kv_heads
    score_scale = head_dim ** (-0.5)
    query_f32 = queries.astype(jnp.float32).reshape(seq_count, kv_heads, per_kv, head_dim)
    keys_f32 = cache[..., :head_dim].astype(jnp.float32)
    vals_f32 = cache[..., head_dim:].astype(jnp.float32)
    scores = jnp.einsum('skgd,slkd->skgl', query_f32, keys_f32) * score_scale
    last_index = jnp.broadcast_to((seq_lens - 1).astype(jnp.int32)[:, None, None], (seq_count, head_count, 1))
    last_gate = jnp.take_along_axis(gates, last_index, axis=2)
    gate_bias = (last_gate - gates + gate_new[:, :, None]).reshape(seq_count, kv_heads, per_kv, cache_len)
    live_mask = (jnp.arange(cache_len, dtype=jnp.int32)[None, :] < seq_lens[:, None])[:, None, None, :]
    cached = jnp.where(live_mask, jnp.exp(scores + gate_bias), 0.0)
    own_keys = key_new.astype(jnp.float32).reshape(seq_count, kv_heads, head_dim)
    own_exp = jnp.exp(jnp.einsum('skgd,skd->skg', query_f32, own_keys) * score_scale)
    denominator = lax.optimization_barrier(jnp.sum(cached, axis=-1)) + own_exp
    weight_cache = lax.optimization_barrier((cached / denominator[..., None]).astype(jnp.bfloat16))
    weight_own = lax.optimization_barrier((own_exp / denominator).astype(jnp.bfloat16))
    attended = jnp.einsum('skgl,slkd->skgd', weight_cache.astype(jnp.float32), vals_f32)
    own_vals = value_new.astype(jnp.float32).reshape(seq_count, kv_heads, 1, head_dim)
    attended = attended + weight_own.astype(jnp.float32)[..., None] * own_vals
    return attended.astype(jnp.bfloat16).reshape(seq_count, head_count * head_dim)

def reference(tokens, norm1_gain, query_weight, key_weight, value_weight, forget_weight, forget_bias, out_weight, kv_cache, log_gates, lengths, norm2_gain, routing, route_weight, expert_gate, expert_up, expert_down, dense_gate, dense_up, dense_down, dense_mix):
    normed = rms_scaled(tokens.astype(jnp.float32), norm1_gain).astype(jnp.bfloat16)
    queries = jnp.dot(normed, query_weight, preferred_element_type=jnp.float32).astype(jnp.bfloat16)
    key_new = jnp.dot(normed, key_weight, preferred_element_type=jnp.float32).astype(jnp.bfloat16)
    value_new = jnp.dot(normed, value_weight, preferred_element_type=jnp.float32).astype(jnp.bfloat16)
    gate_new = jax.nn.log_sigmoid(jnp.dot(normed, forget_weight, preferred_element_type=jnp.float32) + forget_bias)
    operands = [queries, key_new, value_new, gate_new, kv_cache, log_gates, lengths]
    grouped = tuple((operand.reshape((N_EP, SEQ_GRP) + operand.shape[1:]) for operand in operands))
    attended = lax.map(attend_group, grouped).reshape(BATCH_SEQUENCES, QUERY_HEADS * HEAD_DIM)
    attn_out = jnp.dot(attended, out_weight, preferred_element_type=jnp.float32).astype(jnp.bfloat16)
    residual = tokens.astype(jnp.float32) + attn_out.astype(jnp.float32)
    hidden_in = lax.optimization_barrier(rms_scaled(residual, norm2_gain).astype(jnp.bfloat16))
    slot_ids, source = jax.vmap(partial(slot_tables, experts=EXPERTS, capacity=CAP))(routing.reshape(N_EP, SEQ_GRP, TOP))
    group_base = (jnp.arange(N_EP, dtype=jnp.int32) * SEQ_GRP)[:, None, None]
    rows_index = jnp.transpose(source + group_base, (1, 0, 2)).reshape(EXPERTS, N_EP * CAP)

    def run_expert(block_args):
        index_row, gate_w, up_w, down_w = block_args
        picked = hidden_in[index_row]
        gate_pre = jnp.dot(picked, gate_w, preferred_element_type=jnp.float32)
        up_pre = jnp.dot(picked, up_w, preferred_element_type=jnp.float32)
        activation = clamped_unit(gate_pre, up_pre).astype(jnp.bfloat16)
        return jnp.dot(activation, down_w, preferred_element_type=jnp.float32).astype(jnp.bfloat16)
    expert_out = lax.map(run_expert, (rows_index, expert_gate, expert_up, expert_down))
    block_of_row = (jnp.arange(BATCH_SEQUENCES, dtype=jnp.int32) // SEQ_GRP)[:, None]
    flat_index = (routing * N_EP + block_of_row) * CAP + slot_ids.reshape(BATCH_SEQUENCES, TOP)
    picked_out = expert_out.reshape(EXPERTS * N_EP * CAP, D)[flat_index.reshape(-1)].reshape(BATCH_SEQUENCES, TOP, D)
    moe_val = lax.optimization_barrier(jnp.sum(route_weight[..., None] * picked_out.astype(jnp.float32), axis=1))
    dense_gate_pre = jnp.dot(hidden_in, dense_gate, preferred_element_type=jnp.float32)
    dense_up_pre = jnp.dot(hidden_in, dense_up, preferred_element_type=jnp.float32)
    dense_act = clamped_unit(dense_gate_pre, dense_up_pre).astype(jnp.bfloat16)
    dense_val = jnp.dot(dense_act, dense_down, preferred_element_type=jnp.float32)
    mix_gate = jax.nn.sigmoid(jnp.dot(hidden_in.astype(jnp.float32), dense_mix, precision=lax.Precision.HIGHEST))
    return (residual + moe_val + mix_gate[:, None] * dense_val).astype(jnp.bfloat16)
```

```python
import jax
import jax.numpy as jnp
from jax import lax
from jax.sharding import PartitionSpec as P

EPS = 1e-05
LIMIT = 7.0
ALPHA = 1.702
LANES = 128
BF16 = jnp.bfloat16
F32 = jnp.float32


def clamped_unit(gate_pre, up_pre):
    capped = jnp.minimum(gate_pre, LIMIT)
    return capped * jax.nn.sigmoid(ALPHA * capped) * (jnp.clip(up_pre, -LIMIT, LIMIT) + 1.0)


def rms_scaled(values, gain_vec):
    return values * lax.rsqrt(jnp.mean(values * values, axis=-1, keepdims=True) + EPS) * gain_vec


def swap_with(values, axis, offset):
    count = lax.axis_size(axis)
    return lax.ppermute(values, axis, [(i, i ^ offset) for i in range(count)])


def stages_of(count):
    groups = []
    bit = 1
    if bit < count:
        groups.append([bit])
        bit *= 2
    while bit < count:
        if 2 * bit < count:
            groups.append([bit, 2 * bit, 3 * bit])
            bit *= 4
        else:
            groups.append([bit])
            bit *= 2
    return groups


def relative_order(values, index, count):
    bit = 1
    while bit < count:
        pairs = values.reshape((count // (2 * bit), 2, bit) + values.shape[1:])
        swapped = jnp.where((index & bit) != 0, pairs[:, ::-1], pairs)
        values = swapped.reshape(values.shape)
        bit *= 2
    return values


def attention(tokens, norm1_gain, query_weight, key_weight, value_weight, forget_weight, forget_bias, kv_cache, log_gates, lengths):
    seq_count = tokens.shape[0]
    local_heads = forget_bias.shape[0]
    kv_local = kv_cache.shape[2]
    head_dim = kv_cache.shape[3] // 2
    per_kv = local_heads // kv_local
    cache_len = kv_cache.shape[1]
    score_scale = head_dim ** (-0.5)
    normed = rms_scaled(tokens.astype(F32), norm1_gain).astype(BF16)
    queries = jnp.dot(normed, query_weight, preferred_element_type=F32).astype(BF16)
    queries = queries.reshape(seq_count, kv_local, per_kv, head_dim)
    key_new = jnp.dot(normed, key_weight, preferred_element_type=F32).astype(BF16)
    key_new = key_new.reshape(seq_count, kv_local, head_dim)
    value_new = jnp.dot(normed, value_weight, preferred_element_type=F32).astype(BF16)
    value_new = value_new.reshape(seq_count, kv_local, head_dim)
    gate_new = jax.nn.log_sigmoid(
        jnp.dot(normed, forget_weight, preferred_element_type=F32) + forget_bias
    )
    scores = (
        jnp.einsum("skgd,slkd->skgl", queries, kv_cache[..., :head_dim], preferred_element_type=F32)
        * score_scale
    )
    places = jnp.arange(cache_len, dtype=jnp.int32)[None, None, :]
    last_gate = jnp.sum(
        jnp.where(places == (lengths - 1)[:, None, None], log_gates, 0.0), axis=2, keepdims=True
    )
    gate_bias = (last_gate - log_gates + gate_new[:, :, None]).reshape(
        seq_count, kv_local, per_kv, cache_len
    )
    live_mask = (places < lengths[:, None, None])[:, :, None, :]
    cached = jnp.where(live_mask, jnp.exp(scores + gate_bias), 0.0)
    own_exp = jnp.exp(
        jnp.einsum("skgd,skd->skg", queries, key_new, preferred_element_type=F32) * score_scale
    )
    denominator = jnp.sum(cached, axis=-1) + own_exp
    weight_cache = (cached / denominator[..., None]).astype(BF16)
    weight_own = (own_exp / denominator).astype(BF16)
    attended = jnp.einsum(
        "skgl,slkd->skgd", weight_cache, kv_cache[..., head_dim:], preferred_element_type=F32
    )
    attended = attended + weight_own.astype(F32)[..., None] * value_new.astype(F32)[:, :, None, :]
    return attended.astype(BF16).reshape(seq_count, local_heads * head_dim)


def two_halves(values):
    high = lax.reduce_precision(values, 8, 7)
    return high.astype(BF16), (values - high).astype(BF16)


def on_device(
    tokens,
    norm1_gain,
    query_weight,
    key_weight,
    value_weight,
    forget_weight,
    forget_bias,
    out_weight,
    kv_cache,
    log_gates,
    lengths,
    norm2_gain,
    routing,
    route_weight,
    expert_gate,
    expert_up,
    expert_down,
    dense_gate,
    dense_up,
    dense_down,
    dense_mix,
):
    seq_count, width = tokens.shape
    tp_count = lax.axis_size("tp")
    ep_count = lax.axis_size("ep")
    tp_index = lax.axis_index("tp")
    ep_index = lax.axis_index("ep")
    own = seq_count // tp_count
    outer = tp_count // 2
    experts = expert_gate.shape[0] * ep_count

    attended = attention(
        tokens, norm1_gain, query_weight, key_weight, value_weight,
        forget_weight, forget_bias, kv_cache, log_gates, lengths,
    )

    def grouped(values):
        ordered = relative_order(values.reshape((tp_count, own) + values.shape[1:]), tp_index, tp_count)
        return ordered.reshape((outer, 2, own) + values.shape[1:])

    chosen = routing[:, :, None] == jnp.arange(experts, dtype=jnp.int32)[None, None, :]
    weights = jnp.sum(jnp.where(chosen, route_weight[:, :, None], 0.0), axis=1)
    weights = grouped(weights)[:, 0].reshape(outer * own, experts)
    tokens_near = grouped(tokens)[:, 0].astype(F32)

    attended = grouped(attended).reshape(seq_count, -1)
    partial = jnp.dot(attended, out_weight, preferred_element_type=F32)
    partial = partial.reshape(outer, 2, own, width)
    total = partial[:, 0] + swap_with(partial[:, 1].astype(BF16), "tp", 1).astype(F32)
    for (offset,) in [[1 << b] for b in range((outer - 1).bit_length())]:
        rounded = total.astype(BF16)
        received = swap_with(rounded, "tp", 2 * offset)
        received = received.reshape((outer // (2 * offset), 2, offset, own, width))[:, ::-1]
        total = rounded.astype(F32) + received.reshape(total.shape).astype(F32)
    residual = (tokens_near + total.astype(BF16).astype(F32)).reshape(outer * own, width)
    hidden_f32 = rms_scaled(residual, norm2_gain)
    hidden = hidden_f32.astype(BF16)
    mix_gate = jax.nn.sigmoid(jnp.sum(hidden.astype(F32) * dense_mix, axis=-1, keepdims=True))
    scales = jnp.concatenate([weights, mix_gate], axis=1)
    side = jnp.concatenate(two_halves(scales), axis=1)
    side_width = -(-side.shape[1] // LANES) * LANES
    side = jnp.pad(side, ((0, 0), (0, side_width - side.shape[1])))
    rows = jnp.concatenate([hidden, side], axis=1)[None]

    for offsets in stages_of(ep_count)[::-1]:
        rows = jnp.concatenate([rows] + [swap_with(rows, "ep", k) for k in offsets], axis=0)
    rows = jnp.stack([rows, swap_with(rows, "tp", 1)])
    total_rows = rows.size // rows.shape[-1]
    rows = rows.reshape(total_rows, width + side_width)

    everyone = rows[:, :width]
    side = rows[:, width:].astype(F32)
    scales = side[:, : experts + 1] + side[:, experts + 1 : 2 * (experts + 1)]
    mix_all = scales[:, experts:]
    units = dense_gate.shape[1] // tp_count
    start = tp_index * units
    acts, downs = [], []
    for j in range(expert_gate.shape[0]):
        here = ep_index * expert_gate.shape[0] + j
        scale = jnp.sum(
            jnp.where(jnp.arange(experts + 1)[None, :] == here, scales, 0.0), axis=1, keepdims=True
        )
        gate_pre = jnp.dot(everyone, expert_gate[j], preferred_element_type=F32)
        up_pre = jnp.dot(everyone, expert_up[j], preferred_element_type=F32)
        acts.append((scale * clamped_unit(gate_pre, up_pre)).astype(BF16))
        downs.append(expert_down[j])
    gate_pre = jnp.dot(
        everyone, lax.dynamic_slice_in_dim(dense_gate, start, units, 1), preferred_element_type=F32
    )
    up_pre = jnp.dot(
        everyone, lax.dynamic_slice_in_dim(dense_up, start, units, 1), preferred_element_type=F32
    )
    acts.append((mix_all * clamped_unit(gate_pre, up_pre)).astype(BF16))
    downs.append(lax.dynamic_slice_in_dim(dense_down, start, units, 0))
    mixed = sum(jnp.dot(a, d, preferred_element_type=F32) for a, d in zip(acts, downs))

    mixed = mixed.reshape(2, ep_count, outer, own, width)
    mixed = mixed[0] + swap_with(mixed[1].astype(BF16), "tp", 1).astype(F32)
    bit = outer // 2
    while bit >= 1:
        received = swap_with(mixed[:, bit : 2 * bit].astype(BF16), "tp", 2 * bit)
        mixed = mixed[:, :bit] + received.astype(F32)
        bit //= 2
    mixed = mixed[:, 0]
    for offsets in stages_of(ep_count):
        mixed = mixed.reshape((len(offsets) + 1, -1) + mixed.shape[1:])
        pieces = [swap_with(mixed[i + 1].astype(BF16), "ep", k) for i, k in enumerate(offsets)]
        mixed = mixed[0] + sum(p.astype(F32) for p in pieces)
    return (residual[:own] + mixed[0]).astype(BF16)


def solution(mesh):
    return jax.shard_map(
        on_device,
        mesh=mesh,
        in_specs=(
            P("ep", None),
            P(),
            P(None, "tp"),
            P(None, "tp"),
            P(None, "tp"),
            P(None, "tp"),
            P("tp"),
            P("tp", None),
            P("ep", None, "tp", None),
            P("ep", "tp", None),
            P("ep"),
            P(),
            P("ep", None),
            P("ep", None),
            P("ep", None, "tp"),
            P("ep", None, "tp"),
            P("ep", "tp", None),
            P(None, "ep"),
            P(None, "ep"),
            P("ep", None),
            P(),
        ),
        out_specs=P(("ep", "tp"), None),
        check_vma=False,
    )
```

```python
import functools

import jax
import jax.numpy as jnp
from jax import lax
from jax.experimental import pallas as pl
from jax.experimental.pallas import tpu as pltpu
from jax.sharding import PartitionSpec as P

EPS = 1e-05
LIMIT = 7.0
ALPHA = 1.702
LANES = 128
ROW_BLOCK = 128
COLUMN_BLOCK = 512
FFN_VMEM = 16 * 1024 * 1024
ATTENTION_VMEM = 16 * 1024 * 1024
LOAD_VMEM = 1024 * 1024
SEQ_BLOCK = 8
LOAD_COST = 4 * 10**9
BF16 = jnp.bfloat16
F32 = jnp.float32


def clamped_unit(gate_pre, up_pre):
    capped = jnp.minimum(gate_pre, LIMIT)
    return capped * jax.nn.sigmoid(ALPHA * capped) * (jnp.clip(up_pre, -LIMIT, LIMIT) + 1.0)


def rms_scaled(values, gain_vec):
    return values * lax.rsqrt(jnp.mean(values * values, axis=-1, keepdims=True) + EPS) * gain_vec


def swap_with(values, axis, offset):
    count = lax.axis_size(axis)
    return lax.ppermute(values, axis, [(i, i ^ offset) for i in range(count)])


def stages_of(count):
    groups = []
    bit = 1
    if bit < count:
        groups.append([bit])
        bit *= 2
    while bit < count:
        if 2 * bit < count:
            groups.append([bit, 2 * bit, 3 * bit])
            bit *= 4
        else:
            groups.append([bit])
            bit *= 2
    return groups


def relative_order(values, index, count):
    bit = 1
    while bit < count:
        pairs = values.reshape((count // (2 * bit), 2, bit) + values.shape[1:])
        swapped = jnp.where((index & bit) != 0, pairs[:, ::-1], pairs)
        values = swapped.reshape(values.shape)
        bit *= 2
    return values


def attention_kernel(
    own, heads, lengths_hbm, bias_hbm, tokens_hbm, gain_hbm, query_hbm, key_hbm, value_hbm, forget_hbm,
    cache_hbm, gates_hbm, out_hbm, keep_ref, send_ref, near_ref,
    tokens_buf, gain_buf, query_buf, pair_buf, forget_buf, cache_buf, gates_buf, out_buf,
    lengths_ref, bias_ref, sems, cache_sems,
):
    seq_count, width = tokens_buf.shape
    cache_len, lanes = cache_buf.shape[1:]
    head_dim = lanes // 2
    rows = seq_count * heads
    tp_count = seq_count // own
    outer = tp_count // 2
    pairs = [
        (tokens_hbm, tokens_buf),
        (gain_hbm, gain_buf),
        (query_hbm, query_buf),
        (key_hbm, pair_buf.at[pl.ds(0, head_dim), :]),
        (value_hbm, pair_buf.at[pl.ds(head_dim, head_dim), :]),
        (forget_hbm, forget_buf),
        (gates_hbm, gates_buf),
        (lengths_hbm, lengths_ref),
        (bias_hbm, bias_ref),
        (out_hbm, out_buf),
    ]
    copies = [pltpu.make_async_copy(src, dst, sems.at[i]) for i, (src, dst) in enumerate(pairs)]
    cache_copies = [
        pltpu.make_async_copy(cache_hbm.at[s], cache_buf.at[s], cache_sems.at[s]) for s in range(seq_count)
    ]
    for copy in copies[:-1]:
        copy.start()
    for copy in cache_copies:
        copy.start()
    copies[-1].start()

    def one_hot(condition):
        return jnp.where(condition, 1.0, 0.0).astype(BF16)

    copies[0].wait()
    copies[1].wait()
    tokens = tokens_buf[...].astype(F32)
    normed = rms_scaled(tokens, gain_buf[...]).astype(BF16)
    spread = one_hot(
        lax.broadcasted_iota(jnp.int32, (rows, seq_count), 0) // heads
        == lax.broadcasted_iota(jnp.int32, (rows, seq_count), 1)
    )
    normed = jnp.dot(spread, normed, preferred_element_type=F32).astype(BF16)
    order = one_hot(
        chosen_rows(seq_count, seq_count, own, outer)
        == lax.broadcasted_iota(jnp.int32, (seq_count, seq_count), 1)
    )
    near_ref[...] = jnp.dot(order, tokens_buf[...], preferred_element_type=F32)[: seq_count // 2]

    transposed = (((1,), (1,)), ((), ()))
    copies[2].wait()
    queries = jnp.dot(normed, query_buf[...], preferred_element_type=F32).astype(BF16).astype(F32)
    copies[3].wait()
    copies[4].wait()
    own_pair = lax.dot_general(normed, pair_buf[...], transposed, preferred_element_type=F32)
    own_pair = own_pair.astype(BF16).astype(F32)
    copies[5].wait()
    copies[7].wait()
    copies[8].wait()
    forget = lax.dot_general(normed, forget_buf[...], transposed, preferred_element_type=F32)

    lane = lax.broadcasted_iota(jnp.int32, (rows, lanes), 1)
    head = lax.rem(lax.broadcasted_iota(jnp.int32, (rows, lanes), 0), heads)
    queries = jnp.where(head == 0, queries, pltpu.roll(queries, head_dim, 1))
    queries = jnp.where(lane < head_dim, queries, 0.0)
    own_score = jnp.sum(queries * own_pair, axis=1, keepdims=True)
    queries = queries.astype(BF16)

    column = lax.broadcasted_iota(jnp.int32, (rows, heads), 1)
    forget_head = lax.rem(lax.broadcasted_iota(jnp.int32, (rows, heads), 0), heads)
    forget = jnp.sum(jnp.where(column == forget_head, forget, 0.0), axis=1, keepdims=True)
    head_one = lax.rem(lax.broadcasted_iota(jnp.int32, (rows, 1), 0), heads)
    forget = forget + jnp.where(head_one == 0, bias_ref[0], bias_ref[1])
    gate_new = jnp.minimum(forget, 0.0) - jnp.log(1.0 + jnp.exp(-jnp.abs(forget)))

    group = SEQ_BLOCK
    span = group * heads
    scale = head_dim ** (-0.5)
    sequence = lax.broadcasted_iota(jnp.int32, (span, 1), 0) // heads
    place = lax.broadcasted_iota(jnp.int32, (span, cache_len), 1)
    copies[6].wait()
    outputs = []
    for first in range(0, seq_count, group):
        at = slice(first * heads, first * heads + span)
        scores = jnp.zeros((span, cache_len), F32)
        length = jnp.zeros((span, 1), jnp.int32)
        for i in range(group):
            cache_copies[first + i].wait()
            found = lax.dot_general(
                queries[at], cache_buf[first + i], transposed, preferred_element_type=F32
            )
            scores = jnp.where(sequence == i, found, scores)
            length = jnp.where(sequence == i, lengths_ref[first + i], length)
        gates = jnp.concatenate([gates_buf[first + i] for i in range(group)], axis=0)
        last = jnp.sum(jnp.where(place == length - 1, gates, 0.0), axis=1, keepdims=True)
        scores = scores * scale + (last - gates + gate_new[at])
        cached = jnp.where(place < length, jnp.exp(scores), 0.0)
        own_exp = jnp.exp(own_score[at] * scale)
        denominator = jnp.sum(cached, axis=1, keepdims=True) + own_exp
        probs = (cached / denominator).astype(BF16)
        probs_own = (own_exp / denominator).astype(BF16).astype(F32)
        mixed = jnp.zeros((span, lanes), F32)
        for i in range(group):
            found = jnp.dot(probs, cache_buf[first + i], preferred_element_type=F32)
            mixed = jnp.where(sequence == i, found, mixed)
        outputs.append(mixed + probs_own * own_pair[at])
    attended = jnp.concatenate(outputs, axis=0)
    attended = jnp.where(head == 0, pltpu.roll(attended, head_dim, 1), attended)
    attended = jnp.where((lane < head_dim) == (head == 0), attended, 0.0).astype(BF16)
    gather = one_hot(
        chosen_rows(seq_count, rows, own, outer)
        == lax.broadcasted_iota(jnp.int32, (seq_count, rows), 1) // heads
    )
    attended = jnp.dot(gather, attended, preferred_element_type=F32).astype(BF16)
    copies[9].wait()
    partial = jnp.dot(attended, out_buf[...], preferred_element_type=F32)
    keep_ref[...] = partial[: seq_count // 2]
    send_ref[...] = partial[seq_count // 2 :].astype(BF16)


def in_hbm(*arrays):
    return [pltpu.with_memory_space_constraint(array, pltpu.HBM) for array in arrays]


def chosen_rows(seq_count, columns, own, outer):
    place = lax.broadcasted_iota(jnp.int32, (seq_count, columns), 0)
    low = place // (outer * own)
    high = lax.rem(place // own, outer)
    owner = lax.axis_index("tp") ^ (high * 2 + low)
    return owner * own + lax.rem(place, own)


def attention(
    tokens, norm1_gain, query_weight, key_weight, value_weight, forget_weight, forget_bias,
    out_weight, kv_cache, log_gates, lengths, own,
):
    seq_count, width = tokens.shape
    heads = forget_bias.shape[0]
    cache_len, kv_local, lanes = kv_cache.shape[1:]
    assert kv_local == 1 and heads == 2 and lanes == LANES
    half = seq_count // 2
    near = pl.BlockSpec(memory_space=pltpu.VMEM)
    far = pl.BlockSpec(memory_space=pl.ANY)
    return pl.pallas_call(
        functools.partial(attention_kernel, own, heads),
        out_shape=(
            pltpu.VMEM((half, width), F32),
            pltpu.VMEM((half, width), BF16),
            pltpu.VMEM((half, width), F32),
        ),
        in_specs=[far] * 11,
        out_specs=(near,) * 3,
        scratch_shapes=[
            pltpu.VMEM((seq_count, width), BF16),
            pltpu.VMEM((1, width), F32),
            pltpu.VMEM(query_weight.shape, BF16),
            pltpu.VMEM((lanes, width), BF16),
            pltpu.VMEM((heads, width), BF16),
            pltpu.VMEM((seq_count, cache_len, lanes), BF16),
            pltpu.VMEM(log_gates.shape, F32),
            pltpu.VMEM(out_weight.shape, BF16),
            pltpu.SMEM((seq_count,), jnp.int32),
            pltpu.SMEM((heads,), F32),
            pltpu.SemaphoreType.DMA((10,)),
            pltpu.SemaphoreType.DMA((seq_count,)),
        ],
        compiler_params=pltpu.CompilerParams(vmem_limit_bytes=ATTENTION_VMEM),
        name="attention",
    )(
        *in_hbm(
            lengths, forget_bias, tokens, norm1_gain.reshape(1, width), query_weight, key_weight.T, value_weight.T, forget_weight.T,
            kv_cache.reshape(seq_count, cache_len, lanes), log_gates, out_weight,
        ),
    )


def load_kernel(count, units, after_ref, *refs):
    del after_ref
    sources, targets, sems = refs[:count], refs[count:-1], refs[-1]
    pairs = list(zip(sources[:3], targets[:3]))
    if count > 3:
        start = pl.multiple_of(lax.axis_index("tp") * units, units)
        here = pl.ds(start, units)
        pairs += [
            (sources[3].at[:, here], targets[3].at[:, pl.ds(0, units)]),
            (sources[4].at[:, here], targets[3].at[:, pl.ds(units, units)]),
            (sources[5].at[here, :], targets[4]),
        ]
    copies = [pltpu.make_async_copy(src, dst, sems.at[i]) for i, (src, dst) in enumerate(pairs)]
    for copy in copies:
        copy.start()
    for copy in copies:
        copy.wait()


def load_weights(after, expert_weights, dense_weights, units):
    width = dense_weights[0].shape[0]
    near = pl.BlockSpec(memory_space=pltpu.VMEM)
    far = pl.BlockSpec(memory_space=pltpu.HBM)
    shapes = [weight.shape for weight in expert_weights]
    sources = list(expert_weights)
    split = units % LANES == 0
    if split:
        shapes += [(width, 2 * units), (units, width)]
        sources += dense_weights
    count = len(sources)
    loaded = pl.pallas_call(
        functools.partial(load_kernel, count, units),
        out_shape=tuple(pltpu.VMEM(shape, BF16) for shape in shapes),
        in_specs=[near] + [far] * count,
        out_specs=(near,) * len(shapes),
        scratch_shapes=[pltpu.SemaphoreType.DMA((count,))],
        compiler_params=pltpu.CompilerParams(vmem_limit_bytes=LOAD_VMEM),
        cost_estimate=pl.CostEstimate(flops=LOAD_COST, bytes_accessed=8 * width * width, transcendentals=0),
        name="load",
    )(after, *in_hbm(*sources))
    if split:
        return list(loaded)
    gate, up, down = dense_weights
    fill = -gate.shape[1] % LANES
    both = jnp.concatenate([jnp.pad(gate, ((0, 0), (0, fill))), jnp.pad(up, ((0, 0), (0, fill)))], axis=1)
    return [*loaded, both, jnp.pad(down, ((0, fill), (0, 0)))]


def ffn_kernel(
    experts, part, rows_ref, gate_ref, up_ref, down_ref, both_ref, dense_down_ref, keep_ref, send_ref
):
    local, width = gate_ref.shape[:2]
    units = dense_down_ref.shape[0]
    half = rows_ref.shape[0] // 2
    first = lax.axis_index("ep") * local

    def products(at):
        values = rows_ref[at, :width]
        side = rows_ref[at, width:].astype(F32)
        lane = lax.broadcasted_iota(jnp.int32, side.shape, 1)

        def pick(column):
            hit = (lane == column) | (lane == column + experts + 1)
            return jnp.sum(jnp.where(hit, side, 0.0), axis=1, keepdims=True)

        both = jnp.dot(values, both_ref[...], preferred_element_type=F32)
        act = pick(experts) * clamped_unit(both[:, :units], both[:, units:])
        if part != units:
            unit = lax.broadcasted_iota(jnp.int32, act.shape, 1)
            start = lax.axis_index("tp") * part
            act = jnp.where((unit >= start) & (unit < start + part), act, 0.0)
        acts = [act.astype(BF16)]
        for j in range(local):
            gate_pre = jnp.dot(values, gate_ref[j], preferred_element_type=F32)
            up_pre = jnp.dot(values, up_ref[j], preferred_element_type=F32)
            acts.append((pick(first + j) * clamped_unit(gate_pre, up_pre)).astype(BF16))
        step = min(width, COLUMN_BLOCK)
        for column in range(0, width, step):
            cols = slice(column, column + step)
            mixed = jnp.dot(acts[0], dense_down_ref[:, cols], preferred_element_type=F32)
            for j in range(local):
                mixed = mixed + jnp.dot(acts[1 + j], down_ref[j, :, cols], preferred_element_type=F32)
            yield cols, mixed

    if 2 * half <= ROW_BLOCK:
        for cols, mixed in products(slice(0, 2 * half)):
            keep_ref[:, cols] = mixed[:half]
            send_ref[:, cols] = mixed[half:].astype(BF16)
        return
    block = min(half, ROW_BLOCK)

    @pl.loop(0, half // block)
    def _(index):
        at = pl.ds(pl.multiple_of(index * block, block), block)
        for cols, mixed in products(at):
            keep_ref[at, cols] = mixed
        for cols, mixed in products(pl.ds(pl.multiple_of(index * block + half, block), block)):
            send_ref[at, cols] = mixed.astype(BF16)


def ffn(rows, weights, experts, part):
    total = rows.shape[0]
    width = weights[0].shape[1]
    near = pl.BlockSpec(memory_space=pltpu.VMEM)
    return pl.pallas_call(
        functools.partial(ffn_kernel, experts, part),
        out_shape=(
            jax.ShapeDtypeStruct((total // 2, width), F32),
            jax.ShapeDtypeStruct((total // 2, width), BF16),
        ),
        in_specs=[near] * 6,
        out_specs=(near, near),
        compiler_params=pltpu.CompilerParams(vmem_limit_bytes=FFN_VMEM),
        name="ffn",
    )(rows, *weights)


def two_halves(values):
    high = lax.reduce_precision(values, 8, 7)
    return high.astype(BF16), (values - high).astype(BF16)


def on_device(
    tokens,
    norm1_gain,
    query_weight,
    key_weight,
    value_weight,
    forget_weight,
    forget_bias,
    out_weight,
    kv_cache,
    log_gates,
    lengths,
    norm2_gain,
    routing,
    route_weight,
    expert_gate,
    expert_up,
    expert_down,
    dense_gate,
    dense_up,
    dense_down,
    dense_mix,
):
    seq_count, width = tokens.shape
    tp_count = lax.axis_size("tp")
    ep_count = lax.axis_size("ep")
    tp_index = lax.axis_index("tp")
    ep_index = lax.axis_index("ep")
    own = seq_count // tp_count
    outer = tp_count // 2
    experts = expert_gate.shape[0] * ep_count

    keep, sent, tokens_near = attention(
        tokens, norm1_gain, query_weight, key_weight, value_weight, forget_weight, forget_bias,
        out_weight, kv_cache, log_gates, lengths, own,
    )

    def grouped(values):
        ordered = relative_order(values.reshape((tp_count, own) + values.shape[1:]), tp_index, tp_count)
        return ordered.reshape((outer, 2, own) + values.shape[1:])

    chosen = routing[:, :, None] == jnp.arange(experts, dtype=jnp.int32)[None, None, :]
    weights = jnp.sum(jnp.where(chosen, route_weight[:, :, None], 0.0), axis=1)
    weights = grouped(weights)[:, 0].reshape(outer * own, experts)
    total = (keep + swap_with(sent, "tp", 1).astype(F32)).reshape(outer, own, width)
    for (offset,) in [[1 << b] for b in range((outer - 1).bit_length())]:
        rounded = total.astype(BF16)
        received = swap_with(rounded, "tp", 2 * offset)
        received = received.reshape((outer // (2 * offset), 2, offset, own, width))[:, ::-1]
        total = rounded.astype(F32) + received.reshape(total.shape).astype(F32)
    residual = tokens_near + total.astype(BF16).astype(F32).reshape(outer * own, width)
    hidden_f32 = rms_scaled(residual, norm2_gain)
    hidden = hidden_f32.astype(BF16)
    mix_gate = jax.nn.sigmoid(jnp.sum(hidden.astype(F32) * dense_mix, axis=-1, keepdims=True))
    scales = jnp.concatenate([weights, mix_gate], axis=1)
    side = jnp.concatenate(two_halves(scales), axis=1)
    side_width = -(-side.shape[1] // LANES) * LANES
    side = jnp.pad(side, ((0, 0), (0, side_width - side.shape[1])))
    rows = jnp.concatenate([hidden, side], axis=1)[None]
    units = dense_gate.shape[1] // tp_count
    weights_near = load_weights(
        side, [expert_gate, expert_up, expert_down], [dense_gate, dense_up, dense_down], units
    )

    for step, offsets in enumerate(stages_of(ep_count)[::-1]):
        if step == 1:
            rows, *weights_near = lax.optimization_barrier((rows, *weights_near))
        rows = jnp.concatenate([rows] + [swap_with(rows, "ep", k) for k in offsets], axis=0)
    rows = jnp.stack([rows, swap_with(rows, "tp", 1)])
    total_rows = rows.size // rows.shape[-1]
    rows = rows.reshape(total_rows, width + side_width)

    keep, sent = ffn(rows, weights_near, experts, units)

    mixed = (keep + swap_with(sent, "tp", 1).astype(F32)).reshape(ep_count, outer, own, width)
    bit = outer // 2
    while bit >= 1:
        received = swap_with(mixed[:, bit : 2 * bit].astype(BF16), "tp", 2 * bit)
        mixed = mixed[:, :bit] + received.astype(F32)
        bit //= 2
    mixed = mixed[:, 0]
    for offsets in stages_of(ep_count):
        mixed = mixed.reshape((len(offsets) + 1, -1) + mixed.shape[1:])
        pieces = [swap_with(mixed[i + 1].astype(BF16), "ep", k) for i, k in enumerate(offsets)]
        mixed = mixed[0] + sum(p.astype(F32) for p in pieces)
    return (residual[:own] + mixed[0]).astype(BF16)


def solution(mesh):
    return jax.shard_map(
        on_device,
        mesh=mesh,
        in_specs=(
            P("ep", None),
            P(),
            P(None, "tp"),
            P(None, "tp"),
            P(None, "tp"),
            P(None, "tp"),
            P("tp"),
            P("tp", None),
            P("ep", None, "tp", None),
            P("ep", "tp", None),
            P("ep"),
            P(),
            P("ep", None),
            P("ep", None),
            P("ep", None, "tp"),
            P("ep", None, "tp"),
            P("ep", "tp", None),
            P(None, "ep"),
            P(None, "ep"),
            P("ep", None),
            P(),
        ),
        out_specs=P(("ep", "tp"), None),
        check_vma=False,
    )
```

```python
import functools

import jax
import jax.numpy as jnp
from jax import lax
from jax.experimental import pallas as pl
from jax.experimental.pallas import tpu as pltpu
from jax.sharding import PartitionSpec as P

EPS = 1e-05
LIMIT = 7.0
ALPHA = 1.702
LANES = 128
ROW_BLOCK = 128
COLUMN_BLOCK = 512
FFN_VMEM = 16 * 1024 * 1024
ATTENTION_VMEM = 16 * 1024 * 1024
LOAD_VMEM = 1024 * 1024
SEQ_BLOCK = 8
LOAD_COST = 4 * 10**9
BF16 = jnp.bfloat16
F32 = jnp.float32


def clamped_unit(gate_pre, up_pre):
    capped = jnp.minimum(gate_pre, LIMIT)
    return capped * jax.nn.sigmoid(ALPHA * capped) * (jnp.clip(up_pre, -LIMIT, LIMIT) + 1.0)


def rms_scaled(values, gain_vec):
    return values * lax.rsqrt(jnp.mean(values * values, axis=-1, keepdims=True) + EPS) * gain_vec


def swap_with(values, axis, offset):
    count = lax.axis_size(axis)
    return lax.ppermute(values, axis, [(i, i ^ offset) for i in range(count)])


def swap_both(values, ep_offset, tp_offset):
    ep_count, tp_count = lax.axis_size("ep"), lax.axis_size("tp")
    pairs = [
        (e * tp_count + t, (e ^ ep_offset) * tp_count + (t ^ tp_offset))
        for e in range(ep_count)
        for t in range(tp_count)
    ]
    return lax.ppermute(values, ("ep", "tp"), pairs)


def stages_of(count):
    groups = []
    bit = 1
    if bit < count:
        groups.append([bit])
        bit *= 2
    while bit < count:
        if 2 * bit < count:
            groups.append([bit, 2 * bit, 3 * bit])
            bit *= 4
        else:
            groups.append([bit])
            bit *= 2
    return groups


def relative_order(values, index, count):
    bit = 1
    while bit < count:
        pairs = values.reshape((count // (2 * bit), 2, bit) + values.shape[1:])
        swapped = jnp.where((index & bit) != 0, pairs[:, ::-1], pairs)
        values = swapped.reshape(values.shape)
        bit *= 2
    return values


def attention_kernel(
    own, heads, lengths_hbm, bias_hbm, tokens_hbm, gain_hbm, query_hbm, key_hbm, value_hbm, forget_hbm,
    cache_hbm, gates_hbm, out_hbm, keep_ref, send_ref, near_ref,
    tokens_buf, gain_buf, query_buf, pair_buf, forget_buf, cache_buf, gates_buf, out_buf,
    lengths_ref, bias_ref, sems, cache_sems,
):
    seq_count, width = tokens_buf.shape
    cache_len, lanes = cache_buf.shape[1:]
    head_dim = lanes // 2
    rows = seq_count * heads
    tp_count = seq_count // own
    outer = tp_count // 2
    pairs = [
        (tokens_hbm, tokens_buf),
        (gain_hbm, gain_buf),
        (query_hbm, query_buf),
        (key_hbm, pair_buf.at[pl.ds(0, head_dim), :]),
        (value_hbm, pair_buf.at[pl.ds(head_dim, head_dim), :]),
        (forget_hbm, forget_buf),
        (gates_hbm, gates_buf),
        (lengths_hbm, lengths_ref),
        (bias_hbm, bias_ref),
        (out_hbm, out_buf),
    ]
    copies = [pltpu.make_async_copy(src, dst, sems.at[i]) for i, (src, dst) in enumerate(pairs)]
    cache_copies = [
        pltpu.make_async_copy(cache_hbm.at[s], cache_buf.at[s], cache_sems.at[s]) for s in range(seq_count)
    ]
    for copy in copies[:-1]:
        copy.start()

    def one_hot(condition):
        return jnp.where(condition, 1.0, 0.0).astype(BF16)

    copies[0].wait()
    copies[1].wait()
    for copy in cache_copies:
        copy.start()
    copies[-1].start()
    tokens = tokens_buf[...].astype(F32)
    normed = rms_scaled(tokens, gain_buf[...]).astype(BF16)
    spread = one_hot(
        lax.broadcasted_iota(jnp.int32, (rows, seq_count), 0) // heads
        == lax.broadcasted_iota(jnp.int32, (rows, seq_count), 1)
    )
    normed = jnp.dot(spread, normed, preferred_element_type=F32).astype(BF16)
    order = one_hot(
        chosen_rows(seq_count, seq_count, own, outer)
        == lax.broadcasted_iota(jnp.int32, (seq_count, seq_count), 1)
    )
    near_ref[...] = jnp.dot(order, tokens_buf[...], preferred_element_type=F32)[: seq_count // 2]

    transposed = (((1,), (1,)), ((), ()))
    copies[2].wait()
    queries = jnp.dot(normed, query_buf[...], preferred_element_type=F32).astype(BF16).astype(F32)
    copies[3].wait()
    copies[4].wait()
    own_pair = lax.dot_general(normed, pair_buf[...], transposed, preferred_element_type=F32)
    own_pair = own_pair.astype(BF16).astype(F32)
    copies[5].wait()
    copies[7].wait()
    copies[8].wait()
    forget = lax.dot_general(normed, forget_buf[...], transposed, preferred_element_type=F32)

    lane = lax.broadcasted_iota(jnp.int32, (rows, lanes), 1)
    head = lax.rem(lax.broadcasted_iota(jnp.int32, (rows, lanes), 0), heads)
    queries = jnp.where(head == 0, queries, pltpu.roll(queries, head_dim, 1))
    queries = jnp.where(lane < head_dim, queries, 0.0)
    own_score = jnp.sum(queries * own_pair, axis=1, keepdims=True)
    queries = queries.astype(BF16)

    column = lax.broadcasted_iota(jnp.int32, (rows, heads), 1)
    forget_head = lax.rem(lax.broadcasted_iota(jnp.int32, (rows, heads), 0), heads)
    forget = jnp.sum(jnp.where(column == forget_head, forget, 0.0), axis=1, keepdims=True)
    head_one = lax.rem(lax.broadcasted_iota(jnp.int32, (rows, 1), 0), heads)
    forget = forget + jnp.where(head_one == 0, bias_ref[0], bias_ref[1])
    gate_new = jnp.minimum(forget, 0.0) - jnp.log(1.0 + jnp.exp(-jnp.abs(forget)))

    group = SEQ_BLOCK
    span = group * heads
    scale = head_dim ** (-0.5)
    sequence = lax.broadcasted_iota(jnp.int32, (span, 1), 0) // heads
    place = lax.broadcasted_iota(jnp.int32, (span, cache_len), 1)
    copies[6].wait()
    outputs = []
    for first in range(0, seq_count, group):
        at = slice(first * heads, first * heads + span)
        scores = jnp.zeros((span, cache_len), F32)
        length = jnp.zeros((span, 1), jnp.int32)
        for i in range(group):
            cache_copies[first + i].wait()
        for i in range(group):
            found = lax.dot_general(
                queries[at], cache_buf[first + i], transposed, preferred_element_type=F32
            )
            scores = jnp.where(sequence == i, found, scores)
            length = jnp.where(sequence == i, lengths_ref[first + i], length)
        gates = jnp.concatenate([gates_buf[first + i] for i in range(group)], axis=0)
        last = jnp.sum(jnp.where(place == length - 1, gates, 0.0), axis=1, keepdims=True)
        scores = scores * scale + (last - gates + gate_new[at])
        cached = jnp.where(place < length, jnp.exp(scores), 0.0)
        own_exp = jnp.exp(own_score[at] * scale)
        denominator = jnp.sum(cached, axis=1, keepdims=True) + own_exp
        probs = (cached / denominator).astype(BF16)
        probs_own = (own_exp / denominator).astype(BF16).astype(F32)
        mixed = jnp.zeros((span, lanes), F32)
        for i in range(group):
            found = jnp.dot(probs, cache_buf[first + i], preferred_element_type=F32)
            mixed = jnp.where(sequence == i, found, mixed)
        outputs.append(mixed + probs_own * own_pair[at])
    attended = jnp.concatenate(outputs, axis=0)
    attended = jnp.where(head == 0, pltpu.roll(attended, head_dim, 1), attended)
    attended = jnp.where((lane < head_dim) == (head == 0), attended, 0.0).astype(BF16)
    gather = one_hot(
        chosen_rows(seq_count, rows, own, outer)
        == lax.broadcasted_iota(jnp.int32, (seq_count, rows), 1) // heads
    )
    attended = jnp.dot(gather, attended, preferred_element_type=F32).astype(BF16)
    copies[9].wait()
    partial = jnp.dot(attended, out_buf[...], preferred_element_type=F32)
    keep_ref[...] = partial[: seq_count // 2]
    send_ref[...] = partial[seq_count // 2 :].astype(BF16)


def in_hbm(*arrays):
    return [pltpu.with_memory_space_constraint(array, pltpu.HBM) for array in arrays]


def chosen_rows(seq_count, columns, own, outer):
    place = lax.broadcasted_iota(jnp.int32, (seq_count, columns), 0)
    low = place // (outer * own)
    high = lax.rem(place // own, outer)
    owner = lax.axis_index("tp") ^ (high * 2 + low)
    return owner * own + lax.rem(place, own)


def attention(
    tokens, norm1_gain, query_weight, key_weight, value_weight, forget_weight, forget_bias,
    out_weight, kv_cache, log_gates, lengths, own,
):
    seq_count, width = tokens.shape
    heads = forget_bias.shape[0]
    cache_len, kv_local, lanes = kv_cache.shape[1:]
    assert kv_local == 1 and heads == 2 and lanes == LANES
    half = seq_count // 2
    near = pl.BlockSpec(memory_space=pltpu.VMEM)
    far = pl.BlockSpec(memory_space=pl.ANY)
    return pl.pallas_call(
        functools.partial(attention_kernel, own, heads),
        out_shape=(
            pltpu.VMEM((half, width), F32),
            pltpu.VMEM((half, width), BF16),
            pltpu.VMEM((half, width), F32),
        ),
        in_specs=[far] * 11,
        out_specs=(near,) * 3,
        scratch_shapes=[
            pltpu.VMEM((seq_count, width), BF16),
            pltpu.VMEM((1, width), F32),
            pltpu.VMEM(query_weight.shape, BF16),
            pltpu.VMEM((lanes, width), BF16),
            pltpu.VMEM((heads, width), BF16),
            pltpu.VMEM((seq_count, cache_len, lanes), BF16),
            pltpu.VMEM(log_gates.shape, F32),
            pltpu.VMEM(out_weight.shape, BF16),
            pltpu.SMEM((seq_count,), jnp.int32),
            pltpu.SMEM((heads,), F32),
            pltpu.SemaphoreType.DMA((10,)),
            pltpu.SemaphoreType.DMA((seq_count,)),
        ],
        compiler_params=pltpu.CompilerParams(vmem_limit_bytes=ATTENTION_VMEM),
        name="attention",
    )(
        *in_hbm(
            lengths, forget_bias, tokens, norm1_gain.reshape(1, width), query_weight, key_weight.T, value_weight.T, forget_weight.T,
            kv_cache.reshape(seq_count, cache_len, lanes), log_gates, out_weight,
        ),
    )


def load_kernel(count, units, after_ref, *refs):
    del after_ref
    sources, targets, sems = refs[:count], refs[count:-1], refs[-1]
    pairs = list(zip(sources[:3], targets[:3]))
    if count > 3:
        start = pl.multiple_of(lax.axis_index("tp") * units, units)
        here = pl.ds(start, units)
        pairs += [
            (sources[3].at[:, here], targets[3].at[:, pl.ds(0, units)]),
            (sources[4].at[:, here], targets[3].at[:, pl.ds(units, units)]),
            (sources[5].at[here, :], targets[4]),
        ]
    copies = [pltpu.make_async_copy(src, dst, sems.at[i]) for i, (src, dst) in enumerate(pairs)]
    for copy in copies:
        copy.start()
    for copy in copies:
        copy.wait()


def load_weights(after, expert_weights, dense_weights, units):
    width = dense_weights[0].shape[0]
    near = pl.BlockSpec(memory_space=pltpu.VMEM)
    far = pl.BlockSpec(memory_space=pltpu.HBM)
    shapes = [weight.shape for weight in expert_weights]
    sources = list(expert_weights)
    split = units % LANES == 0
    if split:
        shapes += [(width, 2 * units), (units, width)]
        sources += dense_weights
    count = len(sources)
    loaded = pl.pallas_call(
        functools.partial(load_kernel, count, units),
        out_shape=tuple(pltpu.VMEM(shape, BF16) for shape in shapes),
        in_specs=[near] + [far] * count,
        out_specs=(near,) * len(shapes),
        scratch_shapes=[pltpu.SemaphoreType.DMA((count,))],
        compiler_params=pltpu.CompilerParams(vmem_limit_bytes=LOAD_VMEM),
        cost_estimate=pl.CostEstimate(flops=LOAD_COST, bytes_accessed=8 * width * width, transcendentals=0),
        name="load",
    )(after, *in_hbm(*sources))
    if split:
        return list(loaded)
    gate, up, down = dense_weights
    fill = -gate.shape[1] % LANES
    both = jnp.concatenate([jnp.pad(gate, ((0, 0), (0, fill))), jnp.pad(up, ((0, 0), (0, fill)))], axis=1)
    return [*loaded, both, jnp.pad(down, ((0, fill), (0, 0)))]


def ffn_kernel(
    experts, part, rows_ref, gate_ref, up_ref, down_ref, both_ref, dense_down_ref, keep_ref, send_ref
):
    local, width = gate_ref.shape[:2]
    units = dense_down_ref.shape[0]
    half = rows_ref.shape[0] // 2
    first = lax.axis_index("ep") * local

    def products(at):
        values = rows_ref[at, :width]
        side = rows_ref[at, width:].astype(F32)
        lane = lax.broadcasted_iota(jnp.int32, side.shape, 1)

        def pick(column):
            hit = (lane == column) | (lane == column + experts + 1)
            return jnp.sum(jnp.where(hit, side, 0.0), axis=1, keepdims=True)

        both = jnp.dot(values, both_ref[...], preferred_element_type=F32)
        act = pick(experts) * clamped_unit(both[:, :units], both[:, units:])
        if part != units:
            unit = lax.broadcasted_iota(jnp.int32, act.shape, 1)
            start = lax.axis_index("tp") * part
            act = jnp.where((unit >= start) & (unit < start + part), act, 0.0)
        acts = [act.astype(BF16)]
        for j in range(local):
            gate_pre = jnp.dot(values, gate_ref[j], preferred_element_type=F32)
            up_pre = jnp.dot(values, up_ref[j], preferred_element_type=F32)
            acts.append((pick(first + j) * clamped_unit(gate_pre, up_pre)).astype(BF16))
        step = min(width, COLUMN_BLOCK)
        for column in range(0, width, step):
            cols = slice(column, column + step)
            mixed = jnp.dot(acts[0], dense_down_ref[:, cols], preferred_element_type=F32)
            for j in range(local):
                mixed = mixed + jnp.dot(acts[1 + j], down_ref[j, :, cols], preferred_element_type=F32)
            yield cols, mixed

    if 2 * half <= ROW_BLOCK:
        for cols, mixed in products(slice(0, 2 * half)):
            keep_ref[:, cols] = mixed[:half]
            send_ref[:, cols] = mixed[half:].astype(BF16)
        return
    block = min(half, ROW_BLOCK)

    @pl.loop(0, half // block)
    def _(index):
        at = pl.ds(pl.multiple_of(index * block, block), block)
        for cols, mixed in products(at):
            keep_ref[at, cols] = mixed
        for cols, mixed in products(pl.ds(pl.multiple_of(index * block + half, block), block)):
            send_ref[at, cols] = mixed.astype(BF16)


def ffn(rows, weights, experts, part):
    total = rows.shape[0]
    width = weights[0].shape[1]
    near = pl.BlockSpec(memory_space=pltpu.VMEM)
    return pl.pallas_call(
        functools.partial(ffn_kernel, experts, part),
        out_shape=(
            jax.ShapeDtypeStruct((total // 2, width), F32),
            jax.ShapeDtypeStruct((total // 2, width), BF16),
        ),
        in_specs=[near] * 6,
        out_specs=(near, near),
        compiler_params=pltpu.CompilerParams(vmem_limit_bytes=FFN_VMEM),
        name="ffn",
    )(rows, *weights)


def two_halves(values):
    high = lax.reduce_precision(values, 8, 7)
    return high.astype(BF16), (values - high).astype(BF16)


def on_device(
    tokens,
    norm1_gain,
    query_weight,
    key_weight,
    value_weight,
    forget_weight,
    forget_bias,
    out_weight,
    kv_cache,
    log_gates,
    lengths,
    norm2_gain,
    routing,
    route_weight,
    expert_gate,
    expert_up,
    expert_down,
    dense_gate,
    dense_up,
    dense_down,
    dense_mix,
):
    seq_count, width = tokens.shape
    tp_count = lax.axis_size("tp")
    ep_count = lax.axis_size("ep")
    tp_index = lax.axis_index("tp")
    ep_index = lax.axis_index("ep")
    own = seq_count // tp_count
    outer = tp_count // 2
    experts = expert_gate.shape[0] * ep_count

    keep, sent, tokens_near = attention(
        tokens, norm1_gain, query_weight, key_weight, value_weight, forget_weight, forget_bias,
        out_weight, kv_cache, log_gates, lengths, own,
    )

    def grouped(values):
        ordered = relative_order(values.reshape((tp_count, own) + values.shape[1:]), tp_index, tp_count)
        return ordered.reshape((outer, 2, own) + values.shape[1:])

    chosen = routing[:, :, None] == jnp.arange(experts, dtype=jnp.int32)[None, None, :]
    weights = jnp.sum(jnp.where(chosen, route_weight[:, :, None], 0.0), axis=1)
    weights = grouped(weights)[:, 0].reshape(outer * own, experts)
    total = (keep + swap_with(sent, "tp", 1).astype(F32)).reshape(outer, own, width)
    for (offset,) in [[1 << b] for b in range((outer - 1).bit_length())]:
        rounded = total.astype(BF16)
        received = swap_with(rounded, "tp", 2 * offset)
        received = received.reshape((outer // (2 * offset), 2, offset, own, width))[:, ::-1]
        total = rounded.astype(F32) + received.reshape(total.shape).astype(F32)
    residual = tokens_near + total.astype(BF16).astype(F32).reshape(outer * own, width)
    hidden_f32 = rms_scaled(residual, norm2_gain)
    hidden = hidden_f32.astype(BF16)
    mix_gate = jax.nn.sigmoid(jnp.sum(hidden.astype(F32) * dense_mix, axis=-1, keepdims=True))
    scales = jnp.concatenate([weights, mix_gate], axis=1)
    side = jnp.concatenate(two_halves(scales), axis=1)
    side_width = -(-side.shape[1] // LANES) * LANES
    side = jnp.pad(side, ((0, 0), (0, side_width - side.shape[1])))
    rows = jnp.concatenate([hidden, side], axis=1)[None]
    units = dense_gate.shape[1] // tp_count
    weights_near = load_weights(
        side, [expert_gate, expert_up, expert_down], [dense_gate, dense_up, dense_down], units
    )

    for step, offsets in enumerate(stages_of(ep_count)[::-1]):
        if step == 1:
            rows, *weights_near = lax.optimization_barrier((rows, *weights_near))
        rows = jnp.concatenate([rows] + [swap_with(rows, "ep", k) for k in offsets], axis=0)
    rows = jnp.stack([rows, swap_with(rows, "tp", 1)])
    total_rows = rows.size // rows.shape[-1]
    rows = rows.reshape(total_rows, width + side_width)

    keep, sent = ffn(rows, weights_near, experts, units)

    mixed = (keep + swap_with(sent, "tp", 1).astype(F32)).reshape(ep_count, outer, own, width)
    stages = stages_of(ep_count)
    mixed = mixed.reshape(2, ep_count // 2, outer, own, width)
    pieces = [
        swap_both(mixed[e, :, t].astype(BF16), e, 2 * t)
        for e in range(2)
        for t in range(outer)
        if e or t
    ]
    mixed = mixed[0, :, 0] + sum(p.astype(F32) for p in pieces)
    for offsets in stages[1:]:
        mixed = mixed.reshape((len(offsets) + 1, -1) + mixed.shape[1:])
        pieces = [
            swap_with(mixed[i + 1].astype(BF16), "ep", k) for i, k in reversed(list(enumerate(offsets)))
        ]
        mixed = mixed[0] + sum(p.astype(F32) for p in pieces)
    return (residual[:own] + mixed[0]).astype(BF16)


def solution(mesh):
    return jax.shard_map(
        on_device,
        mesh=mesh,
        in_specs=(
            P("ep", None),
            P(),
            P(None, "tp"),
            P(None, "tp"),
            P(None, "tp"),
            P(None, "tp"),
            P("tp"),
            P("tp", None),
            P("ep", None, "tp", None),
            P("ep", "tp", None),
            P("ep"),
            P(),
            P("ep", None),
            P("ep", None),
            P("ep", None, "tp"),
            P("ep", None, "tp"),
            P("ep", "tp", None),
            P(None, "ep"),
            P(None, "ep"),
            P("ep", None),
            P(),
        ),
        out_specs=P(("ep", "tp"), None),
        check_vma=False,
    )
```

```python
import functools

import jax
import jax.numpy as jnp
from jax import lax
from jax.experimental import pallas as pl
from jax.experimental.pallas import tpu as pltpu
from jax.sharding import PartitionSpec as P


EPS = 1e-05
LIMIT = 7.0
ALPHA = 1.702
LANES = 128
ROW_BLOCK = 128
COLUMN_BLOCK = 512
FFN_VMEM = 4 * 1024 * 1024
ATTENTION_VMEM = 16 * 1024 * 1024
LOAD_VMEM = 1024 * 1024
SEQ_BLOCK = 8
NORM_VMEM = 2 * 1024 * 1024
LOAD_COST = 4 * 10**9
BF16 = jnp.bfloat16
F32 = jnp.float32


def clamped_unit(gate_pre, up_pre):
    capped = jnp.minimum(gate_pre, LIMIT)
    return capped * jax.nn.sigmoid(ALPHA * capped) * (jnp.clip(up_pre, -LIMIT, LIMIT) + 1.0)


def rms_scaled(values, gain_vec):
    return values * lax.rsqrt(jnp.mean(values * values, axis=-1, keepdims=True) + EPS) * gain_vec


def swap_with(values, axis, offset):
    count = lax.axis_size(axis)
    return lax.ppermute(values, axis, [(i, i ^ offset) for i in range(count)])


def swap_both(values, ep_offset, tp_offset):
    ep_count, tp_count = lax.axis_size("ep"), lax.axis_size("tp")
    pairs = [
        (e * tp_count + t, (e ^ ep_offset) * tp_count + (t ^ tp_offset))
        for e in range(ep_count)
        for t in range(tp_count)
    ]
    return lax.ppermute(values, ("ep", "tp"), pairs)


def stages_of(count):
    groups = []
    bit = 1
    if bit < count:
        groups.append([bit])
        bit *= 2
    while bit < count:
        if 2 * bit < count:
            groups.append([bit, 2 * bit, 3 * bit])
            bit *= 4
        else:
            groups.append([bit])
            bit *= 2
    return groups


def relative_order(values, index, count):
    bit = 1
    while bit < count:
        pairs = values.reshape((count // (2 * bit), 2, bit) + values.shape[1:])
        swapped = jnp.where((index & bit) != 0, pairs[:, ::-1], pairs)
        values = swapped.reshape(values.shape)
        bit *= 2
    return values


def attention_kernel(
    own, heads, lengths_hbm, bias_hbm, tokens_hbm, gain_hbm, query_hbm, key_hbm, value_hbm, forget_hbm,
    cache_hbm, gates_hbm, out_hbm, keep_ref, send_ref, near_ref,
    tokens_buf, gain_buf, query_buf, pair_buf, forget_buf, cache_buf, gates_buf, out_buf,
    lengths_ref, bias_ref, sems, cache_sems,
):
    seq_count, _ = tokens_buf.shape
    cache_len, lanes = cache_buf.shape[1:]
    head_dim = lanes // 2
    rows = seq_count * heads
    tp_count = seq_count // own
    outer = tp_count // 2
    pairs = [
        (tokens_hbm, tokens_buf),
        (gain_hbm, gain_buf),
        (query_hbm, query_buf),
        (key_hbm, pair_buf.at[pl.ds(0, head_dim), :]),
        (value_hbm, pair_buf.at[pl.ds(head_dim, head_dim), :]),
        (forget_hbm, forget_buf),
        (gates_hbm, gates_buf),
        (lengths_hbm, lengths_ref),
        (bias_hbm, bias_ref),
        (out_hbm, out_buf),
    ]
    copies = [pltpu.make_async_copy(src, dst, sems.at[i]) for i, (src, dst) in enumerate(pairs)]
    cache_copies = [
        pltpu.make_async_copy(cache_hbm.at[s], cache_buf.at[s], cache_sems.at[s]) for s in range(seq_count)
    ]
    for copy in copies[:-1]:
        copy.start()

    def one_hot(condition):
        return jnp.where(condition, 1.0, 0.0).astype(BF16)

    copies[0].wait()
    copies[1].wait()
    for copy in cache_copies:
        copy.start()
    copies[-1].start()
    tokens = tokens_buf[...].astype(F32)
    normed = rms_scaled(tokens, gain_buf[...]).astype(BF16)
    spread = one_hot(
        lax.broadcasted_iota(jnp.int32, (rows, seq_count), 0) // heads
        == lax.broadcasted_iota(jnp.int32, (rows, seq_count), 1)
    )
    normed = jnp.dot(spread, normed, preferred_element_type=F32).astype(BF16)
    order = one_hot(
        chosen_rows(seq_count, seq_count, own, outer)
        == lax.broadcasted_iota(jnp.int32, (seq_count, seq_count), 1)
    )
    near_ref[...] = jnp.dot(order, tokens_buf[...], preferred_element_type=F32)[: seq_count // 2]

    transposed = (((1,), (1,)), ((), ()))
    copies[2].wait()
    queries = jnp.dot(normed, query_buf[...], preferred_element_type=F32).astype(BF16).astype(F32)
    copies[3].wait()
    copies[4].wait()
    own_pair = lax.dot_general(normed, pair_buf[...], transposed, preferred_element_type=F32)
    own_pair = own_pair.astype(BF16).astype(F32)
    copies[5].wait()
    copies[7].wait()
    copies[8].wait()
    forget = lax.dot_general(normed, forget_buf[...], transposed, preferred_element_type=F32)

    lane = lax.broadcasted_iota(jnp.int32, (rows, lanes), 1)
    head = lax.rem(lax.broadcasted_iota(jnp.int32, (rows, lanes), 0), heads)
    queries = jnp.where(head == 0, queries, pltpu.roll(queries, head_dim, 1))
    queries = jnp.where(lane < head_dim, queries, 0.0)
    own_score = jnp.sum(queries * own_pair, axis=1, keepdims=True)
    queries = queries.astype(BF16)

    column = lax.broadcasted_iota(jnp.int32, (rows, heads), 1)
    forget_head = lax.rem(lax.broadcasted_iota(jnp.int32, (rows, heads), 0), heads)
    forget = jnp.sum(jnp.where(column == forget_head, forget, 0.0), axis=1, keepdims=True)
    head_one = lax.rem(lax.broadcasted_iota(jnp.int32, (rows, 1), 0), heads)
    forget = forget + jnp.where(head_one == 0, bias_ref[0], bias_ref[1])
    gate_new = jnp.minimum(forget, 0.0) - jnp.log(1.0 + jnp.exp(-jnp.abs(forget)))

    group = SEQ_BLOCK
    span = group * heads
    scale = head_dim ** (-0.5)
    sequence = lax.broadcasted_iota(jnp.int32, (span, 1), 0) // heads
    place = lax.broadcasted_iota(jnp.int32, (span, cache_len), 1)
    copies[6].wait()
    outputs = []
    for first in range(0, seq_count, group):
        at = slice(first * heads, first * heads + span)
        scores = jnp.zeros((span, cache_len), F32)
        length = jnp.zeros((span, 1), jnp.int32)
        for i in range(group):
            cache_copies[first + i].wait()
        for i in range(group):
            found = lax.dot_general(
                queries[at], cache_buf[first + i], transposed, preferred_element_type=F32
            )
            scores = jnp.where(sequence == i, found, scores)
            length = jnp.where(sequence == i, lengths_ref[first + i], length)
        gates = jnp.concatenate([gates_buf[first + i] for i in range(group)], axis=0)
        last = jnp.sum(jnp.where(place == length - 1, gates, 0.0), axis=1, keepdims=True)
        scores = scores * scale + (last - gates + gate_new[at])
        cached = jnp.where(place < length, jnp.exp(scores), 0.0)
        own_exp = jnp.exp(own_score[at] * scale)
        denominator = jnp.sum(cached, axis=1, keepdims=True) + own_exp
        probs = (cached / denominator).astype(BF16)
        probs_own = (own_exp / denominator).astype(BF16).astype(F32)
        mixed = jnp.zeros((span, lanes), F32)
        for i in range(group):
            found = jnp.dot(probs, cache_buf[first + i], preferred_element_type=F32)
            mixed = jnp.where(sequence == i, found, mixed)
        outputs.append(mixed + probs_own * own_pair[at])
    attended = jnp.concatenate(outputs, axis=0)
    attended = jnp.where(head == 0, pltpu.roll(attended, head_dim, 1), attended)
    attended = jnp.where((lane < head_dim) == (head == 0), attended, 0.0).astype(BF16)
    gather = one_hot(
        chosen_rows(seq_count, rows, own, outer)
        == lax.broadcasted_iota(jnp.int32, (seq_count, rows), 1) // heads
    )
    attended = jnp.dot(gather, attended, preferred_element_type=F32).astype(BF16)
    copies[9].wait()
    partial = jnp.dot(attended, out_buf[...], preferred_element_type=F32)
    keep_ref[...] = partial[: seq_count // 2].astype(BF16)
    send_ref[...] = partial[seq_count // 2 :].astype(BF16)


def in_hbm(*arrays):
    return [pltpu.with_memory_space_constraint(array, pltpu.HBM) for array in arrays]


def chosen_rows(seq_count, columns, own, outer):
    place = lax.broadcasted_iota(jnp.int32, (seq_count, columns), 0)
    low = place // (outer * own)
    high = lax.rem(place // own, outer)
    owner = lax.axis_index("tp") ^ (high * 2 + low)
    return owner * own + lax.rem(place, own)


def attention(
    tokens, norm1_gain, query_weight, key_weight, value_weight, forget_weight, forget_bias,
    out_weight, kv_cache, log_gates, lengths, own,
):
    seq_count, width = tokens.shape
    heads = forget_bias.shape[0]
    cache_len, kv_local, lanes = kv_cache.shape[1:]
    assert kv_local == 1 and heads == 2 and lanes == LANES
    half = seq_count // 2
    near = pl.BlockSpec(memory_space=pltpu.VMEM)
    far = pl.BlockSpec(memory_space=pl.ANY)
    return pl.pallas_call(
        functools.partial(attention_kernel, own, heads),
        out_shape=(
            pltpu.VMEM((half, width), BF16),
            pltpu.VMEM((half, width), BF16),
            pltpu.VMEM((half, width), F32),
        ),
        in_specs=[far] * 11,
        out_specs=(near,) * 3,
        scratch_shapes=[
            pltpu.VMEM((seq_count, width), BF16),
            pltpu.VMEM((1, width), F32),
            pltpu.VMEM(query_weight.shape, BF16),
            pltpu.VMEM((lanes, width), BF16),
            pltpu.VMEM((heads, width), BF16),
            pltpu.VMEM((seq_count, cache_len, lanes), BF16),
            pltpu.VMEM(log_gates.shape, F32),
            pltpu.VMEM(out_weight.shape, BF16),
            pltpu.SMEM((seq_count,), jnp.int32),
            pltpu.SMEM((heads,), F32),
            pltpu.SemaphoreType.DMA((10,)),
            pltpu.SemaphoreType.DMA((seq_count,)),
        ],
        compiler_params=pltpu.CompilerParams(vmem_limit_bytes=ATTENTION_VMEM),
        name="attention",
    )(
        *in_hbm(
            lengths, forget_bias, tokens, norm1_gain.reshape(1, width), query_weight, key_weight.T, value_weight.T, forget_weight.T,
            kv_cache.reshape(seq_count, cache_len, lanes), log_gates, out_weight,
        ),
    )


def load_kernel(count, units, after_ref, *refs):
    del after_ref
    sources, targets, sems = refs[:count], refs[count:-1], refs[-1]
    pairs = list(zip(sources[:3], targets[:3]))
    if count > 3:
        start = pl.multiple_of(lax.axis_index("tp") * units, units)
        here = pl.ds(start, units)
        pairs += [
            (sources[3].at[:, here], targets[3].at[:, pl.ds(0, units)]),
            (sources[4].at[:, here], targets[3].at[:, pl.ds(units, units)]),
            (sources[5].at[here, :], targets[4]),
        ]
    copies = [pltpu.make_async_copy(src, dst, sems.at[i]) for i, (src, dst) in enumerate(pairs)]
    for copy in copies:
        copy.start()
    for copy in copies:
        copy.wait()


def load_weights(after, expert_weights, dense_weights, units):
    width = dense_weights[0].shape[0]
    near = pl.BlockSpec(memory_space=pltpu.VMEM)
    far = pl.BlockSpec(memory_space=pltpu.HBM)
    shapes = [weight.shape for weight in expert_weights]
    sources = list(expert_weights)
    split = units % LANES == 0
    if split:
        shapes += [(width, 2 * units), (units, width)]
        sources += dense_weights
    count = len(sources)
    loaded = pl.pallas_call(
        functools.partial(load_kernel, count, units),
        out_shape=tuple(pltpu.VMEM(shape, BF16) for shape in shapes),
        in_specs=[near] + [far] * count,
        out_specs=(near,) * len(shapes),
        scratch_shapes=[pltpu.SemaphoreType.DMA((count,))],
        compiler_params=pltpu.CompilerParams(vmem_limit_bytes=LOAD_VMEM),
        cost_estimate=pl.CostEstimate(flops=LOAD_COST, bytes_accessed=8 * width * width, transcendentals=0),
        name="load",
    )(after, *in_hbm(*sources))
    if split:
        return list(loaded)
    gate, up, down = dense_weights
    fill = -gate.shape[1] % LANES
    both = jnp.concatenate([jnp.pad(gate, ((0, 0), (0, fill))), jnp.pad(up, ((0, 0), (0, fill)))], axis=1)
    return [*loaded, both, jnp.pad(down, ((0, fill), (0, 0)))]


def ffn_kernel(
    experts, part, rows_ref, gate_ref, up_ref, down_ref, both_ref, dense_down_ref, keep_ref, send_ref
):
    local, width = gate_ref.shape[:2]
    units = dense_down_ref.shape[0]
    half = rows_ref.shape[0] // 2
    first = lax.axis_index("ep") * local

    def products(at):
        values = rows_ref[at, :width]
        side = rows_ref[at, width:].astype(F32)
        lane = lax.broadcasted_iota(jnp.int32, side.shape, 1)

        def pick(column):
            hit = (lane == column) | (lane == column + experts + 1)
            return jnp.sum(jnp.where(hit, side, 0.0), axis=1, keepdims=True)

        both = jnp.dot(values, both_ref[...], preferred_element_type=F32)
        act = pick(experts) * clamped_unit(both[:, :units], both[:, units:])
        if part != units:
            unit = lax.broadcasted_iota(jnp.int32, act.shape, 1)
            start = lax.axis_index("tp") * part
            act = jnp.where((unit >= start) & (unit < start + part), act, 0.0)
        acts = [act.astype(BF16)]
        for j in range(local):
            gate_pre = jnp.dot(values, gate_ref[j], preferred_element_type=F32)
            up_pre = jnp.dot(values, up_ref[j], preferred_element_type=F32)
            acts.append((pick(first + j) * clamped_unit(gate_pre, up_pre)).astype(BF16))
        step = min(width, COLUMN_BLOCK)
        for column in range(0, width, step):
            cols = slice(column, column + step)
            mixed = jnp.dot(acts[0], dense_down_ref[:, cols], preferred_element_type=F32)
            for j in range(local):
                mixed = mixed + jnp.dot(acts[1 + j], down_ref[j, :, cols], preferred_element_type=F32)
            yield cols, mixed

    if 2 * half <= ROW_BLOCK:
        for cols, mixed in products(slice(0, 2 * half)):
            keep_ref[:, cols] = mixed[:half]
            send_ref[:, cols] = mixed[half:].astype(BF16)
        return
    block = min(half, ROW_BLOCK)

    @pl.loop(0, half // block)
    def _(index):
        at = pl.ds(pl.multiple_of(index * block, block), block)
        for cols, mixed in products(at):
            keep_ref[at, cols] = mixed
        for cols, mixed in products(pl.ds(pl.multiple_of(index * block + half, block), block)):
            send_ref[at, cols] = mixed.astype(BF16)


def ffn(rows, weights, experts, part):
    total = rows.shape[0]
    width = weights[0].shape[1]
    near = pl.BlockSpec(memory_space=pltpu.VMEM)
    return pl.pallas_call(
        functools.partial(ffn_kernel, experts, part),
        out_shape=(
            jax.ShapeDtypeStruct((total // 2, width), F32),
            jax.ShapeDtypeStruct((total // 2, width), BF16),
        ),
        in_specs=[near] * 6,
        out_specs=(near, near),
        compiler_params=pltpu.CompilerParams(vmem_limit_bytes=FFN_VMEM),
        name="ffn",
    )(rows, *weights)


def fold_kernel(keep_ref, received_ref, stay_ref, send_ref):
    sublane = lax.broadcasted_iota(jnp.int32, (8, keep_ref.shape[1]), 0)
    for row in range(0, keep_ref.shape[0], 16):
        first, second = [
            keep_ref[at : at + 8] + received_ref[at : at + 8].astype(F32) for at in (row, row + 8)
        ]
        at = slice(row // 2, row // 2 + 8)
        stay_ref[at] = jnp.where(sublane < 4, first, pltpu.roll(second, 4, 0)).astype(stay_ref.dtype)
        send_ref[at] = jnp.where(sublane < 4, pltpu.roll(first, 4, 0), second).astype(BF16)


def fold(keep, received, outer, own, stay_type):
    count, width = keep.shape
    if outer != 2 or own != 4 or count % 16:
        total = (keep + received.astype(F32)).reshape(-1, outer, own, width)
        parts = [total[:, t].reshape(-1, width) for t in range(outer)]
        return [parts[0].astype(stay_type)] + [p.astype(BF16) for p in parts[1:]]
    near = pl.BlockSpec(memory_space=pltpu.VMEM)
    return pl.pallas_call(
        fold_kernel,
        out_shape=(
            pltpu.VMEM((count // 2, width), stay_type),
            pltpu.VMEM((count // 2, width), BF16),
        ),
        in_specs=[near] * 2,
        out_specs=(near, near),
        compiler_params=pltpu.CompilerParams(vmem_limit_bytes=NORM_VMEM),
        name="fold",
    )(keep, received)


def norm_kernel(mix_lane, shifts, *refs):
    parts, (tokens_ref, gain_ref, dense_mix_ref, side_ref, rows_ref, residual_ref) = (
        refs[: len(shifts)],
        refs[len(shifts) :],
    )
    norm_body(mix_lane, shifts, parts, tokens_ref, gain_ref, dense_mix_ref, side_ref, rows_ref, residual_ref)


def norm_body(mix_lane, shifts, parts, tokens_ref, gain_ref, dense_mix_ref, side_ref, rows_ref, residual_ref):
    width = tokens_ref.shape[1]
    sums = {}
    for shift, part in zip(shifts, parts):
        sums[shift] = sums.get(shift, 0.0) + part[...].astype(F32)
    total = sums.pop(0)
    for shift, part in sums.items():
        total = total + pltpu.roll(part, shift, 0)
    residual = tokens_ref[...] + total.astype(BF16).astype(F32)
    residual_ref[...] = residual
    hidden = rms_scaled(residual, gain_ref[...]).astype(BF16)
    rows_ref[:, :width] = hidden
    mix = jax.nn.sigmoid(jnp.sum(hidden.astype(F32) * dense_mix_ref[...], axis=1, keepdims=True))
    high = mix.astype(BF16).astype(F32)
    side = side_ref[...]
    lane = lax.broadcasted_iota(jnp.int32, side.shape, 1)
    side = jnp.where(lane == mix_lane, high, side)
    side = jnp.where(lane == 2 * mix_lane + 1, mix - high, side)
    rows_ref[:, width:] = side.astype(BF16)


def norm_rows(parts, shifts, tokens, gain, dense_mix, side, mix_lane):
    count, width = tokens.shape
    near = pl.BlockSpec(memory_space=pltpu.VMEM)
    return pl.pallas_call(
        functools.partial(norm_kernel, mix_lane, tuple(shifts)),
        out_shape=(
            pltpu.VMEM((count, width + side.shape[1]), BF16),
            pltpu.VMEM((count, width), F32),
        ),
        in_specs=[near] * (len(parts) + 4),
        out_specs=(near, near),
        compiler_params=pltpu.CompilerParams(vmem_limit_bytes=NORM_VMEM),
        name="norm",
    )(*parts, tokens, gain.reshape(1, width), dense_mix.reshape(1, width), side)


def on_device(
    tokens,
    norm1_gain,
    query_weight,
    key_weight,
    value_weight,
    forget_weight,
    forget_bias,
    out_weight,
    kv_cache,
    log_gates,
    lengths,
    norm2_gain,
    routing,
    route_weight,
    expert_gate,
    expert_up,
    expert_down,
    dense_gate,
    dense_up,
    dense_down,
    dense_mix,
):
    seq_count, width = tokens.shape
    tp_count = lax.axis_size("tp")
    ep_count = lax.axis_size("ep")
    tp_index = lax.axis_index("tp")
    own = seq_count // tp_count
    outer = tp_count // 2
    experts = expert_gate.shape[0] * ep_count

    keep, sent, tokens_near = attention(
        tokens, norm1_gain, query_weight, key_weight, value_weight, forget_weight, forget_bias,
        out_weight, kv_cache, log_gates, lengths, own,
    )

    def grouped(values):
        ordered = relative_order(values.reshape((tp_count, own) + values.shape[1:]), tp_index, tp_count)
        return ordered.reshape((outer, 2, own) + values.shape[1:])

    chosen = routing[:, :, None] == jnp.arange(experts, dtype=jnp.int32)[None, None, :]
    weights = jnp.sum(jnp.where(chosen, route_weight[:, :, None], 0.0), axis=1)
    weights = grouped(weights)[:, 0].reshape(outer * own, experts)
    parts, shifts = [keep], [0]
    for k in range(1, tp_count):
        part = swap_with(sent if k & 1 else keep, "tp", k)
        turn = k >> 1
        if outer == 2:
            shifts.append(turn * own)
        else:
            blocks = part.reshape(outer, own, width)
            part = jnp.stack([blocks[j ^ turn] for j in range(outer)]).reshape(part.shape)
            shifts.append(0)
        parts.append(part)
    high = lax.reduce_precision(weights, 8, 7)
    none = jnp.zeros((outer * own, 1), F32)
    side = jnp.concatenate([high, none, weights - high, none], axis=1)
    side = jnp.pad(side, ((0, 0), (0, -side.shape[1] % LANES)))
    rows, residual = norm_rows(
        parts, shifts, tokens_near, norm2_gain, dense_mix, side, experts
    )
    units = dense_gate.shape[1] // tp_count
    weights_near = load_weights(
        rows, [expert_gate, expert_up, expert_down], [dense_gate, dense_up, dense_down], units
    )

    stages = stages_of(ep_count)
    for offsets in stages[:0:-1]:
        others = []
        for k in offsets:
            others.append(swap_with(rows, "ep", k))
        rows = jnp.concatenate([rows] + others, axis=0)
    rows, *weights_near = lax.optimization_barrier((rows, *weights_near))

    rows = jnp.concatenate([rows, swap_with(rows, "ep", 1)], axis=0)
    rows = jnp.concatenate([rows, swap_with(rows, "tp", 1)], axis=0)
    keep, sent = ffn(rows, weights_near, experts, units)
    parts = fold(keep, swap_with(sent, "tp", 1), outer, own, F32)
    half = parts[0].shape[0] // 2
    mixed = parts[0][:half]
    pieces = []
    for e in range(2):
        for t in range(outer):
            if e or t:
                part = parts[t][e * half : (e + 1) * half].astype(BF16)
                pieces.append(swap_both(part, e, 2 * t))
    mixed = (mixed + sum(p.astype(F32) for p in pieces)).reshape(ep_count // 2, own, width)
    for offsets in stages[1:]:
        mixed = mixed.reshape((len(offsets) + 1, -1) + mixed.shape[1:])
        pieces = []
        for i, k in enumerate(offsets):
            pieces.append(swap_with(mixed[i + 1].astype(BF16), "ep", k))
        mixed = mixed[0] + sum(p.astype(F32) for p in pieces)
    return (residual[:own] + mixed[0]).astype(BF16)


def solution(mesh):
    return jax.shard_map(
        on_device,
        mesh=mesh,
        in_specs=(
            P("ep", None),
            P(),
            P(None, "tp"),
            P(None, "tp"),
            P(None, "tp"),
            P(None, "tp"),
            P("tp"),
            P("tp", None),
            P("ep", None, "tp", None),
            P("ep", "tp", None),
            P("ep"),
            P(),
            P("ep", None),
            P("ep", None),
            P("ep", None, "tp"),
            P("ep", None, "tp"),
            P("ep", "tp", None),
            P(None, "ep"),
            P(None, "ep"),
            P("ep", None),
            P(),
        ),
        out_specs=P(("ep", "tp"), None),
        check_vma=False,
    )
```

```python
import functools

import jax
import jax.numpy as jnp
from jax import lax
from jax.experimental import pallas as pl
from jax.experimental.pallas import tpu as pltpu
from jax.sharding import PartitionSpec as P


EPS = 1e-05
LIMIT = 7.0
ALPHA = 1.702
LANES = 128
ROW_BLOCK = 128
COLUMN_BLOCK = 512
FFN_VMEM = 4 * 1024 * 1024
ATTENTION_VMEM = 16 * 1024 * 1024
LOAD_VMEM = 1024 * 1024
SEQ_BLOCK = 8
NORM_VMEM = 2 * 1024 * 1024
LOAD_COST = 4 * 10**9
BF16 = jnp.bfloat16
F32 = jnp.float32


def clamped_unit(gate_pre, up_pre):
    capped = jnp.minimum(gate_pre, LIMIT)
    return capped * jax.nn.sigmoid(ALPHA * capped) * (jnp.clip(up_pre, -LIMIT, LIMIT) + 1.0)


def rms_scaled(values, gain_vec):
    return values * lax.rsqrt(jnp.mean(values * values, axis=-1, keepdims=True) + EPS) * gain_vec


def swap_with(values, axis, offset):
    count = lax.axis_size(axis)
    return lax.ppermute(values, axis, [(i, i ^ offset) for i in range(count)])


def swap_both(values, ep_offset, tp_offset):
    ep_count, tp_count = lax.axis_size("ep"), lax.axis_size("tp")
    pairs = [
        (e * tp_count + t, (e ^ ep_offset) * tp_count + (t ^ tp_offset))
        for e in range(ep_count)
        for t in range(tp_count)
    ]
    return lax.ppermute(values, ("ep", "tp"), pairs)


def stages_of(count):
    groups = []
    bit = 1
    if bit < count:
        groups.append([bit])
        bit *= 2
    while bit < count:
        if 2 * bit < count:
            groups.append([bit, 2 * bit, 3 * bit])
            bit *= 4
        else:
            groups.append([bit])
            bit *= 2
    return groups


def relative_order(values, index, count):
    bit = 1
    while bit < count:
        pairs = values.reshape((count // (2 * bit), 2, bit) + values.shape[1:])
        swapped = jnp.where((index & bit) != 0, pairs[:, ::-1], pairs)
        values = swapped.reshape(values.shape)
        bit *= 2
    return values


def attention_kernel(
    own, heads, lengths_hbm, bias_hbm, tokens_hbm, gain_hbm, query_hbm, key_hbm, value_hbm, forget_hbm,
    cache_hbm, gates_hbm, out_hbm, keep_ref, send_ref, near_ref,
    tokens_buf, gain_buf, query_buf, pair_buf, forget_buf, cache_buf, gates_buf, out_buf,
    lengths_ref, bias_ref, sems, cache_sems,
):
    seq_count, _ = tokens_buf.shape
    cache_len, lanes = cache_buf.shape[1:]
    head_dim = lanes // 2
    rows = seq_count * heads
    tp_count = seq_count // own
    outer = tp_count // 2
    pairs = [
        (tokens_hbm, tokens_buf),
        (gain_hbm, gain_buf),
        (query_hbm, query_buf),
        (key_hbm, pair_buf.at[pl.ds(0, head_dim), :]),
        (value_hbm, pair_buf.at[pl.ds(head_dim, head_dim), :]),
        (forget_hbm, forget_buf),
        (gates_hbm, gates_buf),
        (lengths_hbm, lengths_ref),
        (bias_hbm, bias_ref),
        (out_hbm, out_buf),
    ]
    copies = [pltpu.make_async_copy(src, dst, sems.at[i]) for i, (src, dst) in enumerate(pairs)]
    cache_copies = [
        pltpu.make_async_copy(cache_hbm.at[s], cache_buf.at[s], cache_sems.at[s]) for s in range(seq_count)
    ]
    for copy in copies[:-1]:
        copy.start()

    def one_hot(condition):
        return jnp.where(condition, 1.0, 0.0).astype(BF16)

    copies[0].wait()
    copies[1].wait()
    for copy in cache_copies:
        copy.start()
    copies[-1].start()
    tokens = tokens_buf[...].astype(F32)
    normed = rms_scaled(tokens, gain_buf[...]).astype(BF16)
    spread = one_hot(
        lax.broadcasted_iota(jnp.int32, (rows, seq_count), 0) // heads
        == lax.broadcasted_iota(jnp.int32, (rows, seq_count), 1)
    )
    normed = jnp.dot(spread, normed, preferred_element_type=F32).astype(BF16)
    order = one_hot(
        chosen_rows(seq_count, seq_count, own, outer)
        == lax.broadcasted_iota(jnp.int32, (seq_count, seq_count), 1)
    )
    near_ref[...] = jnp.dot(order, tokens_buf[...], preferred_element_type=F32)[: seq_count // 2]

    transposed = (((1,), (1,)), ((), ()))
    copies[2].wait()
    queries = jnp.dot(normed, query_buf[...], preferred_element_type=F32).astype(BF16).astype(F32)
    copies[3].wait()
    copies[4].wait()
    own_pair = lax.dot_general(normed, pair_buf[...], transposed, preferred_element_type=F32)
    own_pair = own_pair.astype(BF16).astype(F32)
    copies[5].wait()
    copies[7].wait()
    copies[8].wait()
    forget = lax.dot_general(normed, forget_buf[...], transposed, preferred_element_type=F32)

    lane = lax.broadcasted_iota(jnp.int32, (rows, lanes), 1)
    head = lax.rem(lax.broadcasted_iota(jnp.int32, (rows, lanes), 0), heads)
    queries = jnp.where(head == 0, queries, pltpu.roll(queries, head_dim, 1))
    queries = jnp.where(lane < head_dim, queries, 0.0)
    own_score = jnp.sum(queries * own_pair, axis=1, keepdims=True)
    queries = queries.astype(BF16)

    column = lax.broadcasted_iota(jnp.int32, (rows, heads), 1)
    forget_head = lax.rem(lax.broadcasted_iota(jnp.int32, (rows, heads), 0), heads)
    forget = jnp.sum(jnp.where(column == forget_head, forget, 0.0), axis=1, keepdims=True)
    head_one = lax.rem(lax.broadcasted_iota(jnp.int32, (rows, 1), 0), heads)
    forget = forget + jnp.where(head_one == 0, bias_ref[0], bias_ref[1])
    gate_new = jnp.minimum(forget, 0.0) - jnp.log(1.0 + jnp.exp(-jnp.abs(forget)))

    group = SEQ_BLOCK
    span = group * heads
    scale = head_dim ** (-0.5)
    sequence = lax.broadcasted_iota(jnp.int32, (span, 1), 0) // heads
    place = lax.broadcasted_iota(jnp.int32, (span, cache_len), 1)
    copies[6].wait()
    outputs = []
    for first in range(0, seq_count, group):
        at = slice(first * heads, first * heads + span)
        scores = jnp.zeros((span, cache_len), F32)
        length = jnp.zeros((span, 1), jnp.int32)
        for i in range(group):
            cache_copies[first + i].wait()
        for i in range(group):
            found = lax.dot_general(
                queries[at], cache_buf[first + i], transposed, preferred_element_type=F32
            )
            scores = jnp.where(sequence == i, found, scores)
            length = jnp.where(sequence == i, lengths_ref[first + i], length)
        gates = jnp.concatenate([gates_buf[first + i] for i in range(group)], axis=0)
        last = jnp.sum(jnp.where(place == length - 1, gates, 0.0), axis=1, keepdims=True)
        scores = scores * scale + (last - gates + gate_new[at])
        cached = jnp.where(place < length, jnp.exp(scores), 0.0)
        own_exp = jnp.exp(own_score[at] * scale)
        denominator = jnp.sum(cached, axis=1, keepdims=True) + own_exp
        probs = (cached / denominator).astype(BF16)
        probs_own = (own_exp / denominator).astype(BF16).astype(F32)
        mixed = jnp.zeros((span, lanes), F32)
        for i in range(group):
            found = jnp.dot(probs, cache_buf[first + i], preferred_element_type=F32)
            mixed = jnp.where(sequence == i, found, mixed)
        outputs.append(mixed + probs_own * own_pair[at])
    attended = jnp.concatenate(outputs, axis=0)
    attended = jnp.where(head == 0, pltpu.roll(attended, head_dim, 1), attended)
    attended = jnp.where((lane < head_dim) == (head == 0), attended, 0.0).astype(BF16)
    gather = one_hot(
        chosen_rows(seq_count, rows, own, outer)
        == lax.broadcasted_iota(jnp.int32, (seq_count, rows), 1) // heads
    )
    attended = jnp.dot(gather, attended, preferred_element_type=F32).astype(BF16)
    copies[9].wait()
    partial = jnp.dot(attended, out_buf[...], preferred_element_type=F32)
    keep_ref[...] = partial[: seq_count // 2].astype(BF16)
    send_ref[...] = partial[seq_count // 2 :].astype(BF16)


def in_hbm(*arrays):
    return [pltpu.with_memory_space_constraint(array, pltpu.HBM) for array in arrays]


def chosen_rows(seq_count, columns, own, outer):
    place = lax.broadcasted_iota(jnp.int32, (seq_count, columns), 0)
    low = place // (outer * own)
    high = lax.rem(place // own, outer)
    owner = lax.axis_index("tp") ^ (high * 2 + low)
    return owner * own + lax.rem(place, own)


def attention(
    tokens, norm1_gain, query_weight, key_weight, value_weight, forget_weight, forget_bias,
    out_weight, kv_cache, log_gates, lengths, own,
):
    seq_count, width = tokens.shape
    heads = forget_bias.shape[0]
    cache_len, kv_local, lanes = kv_cache.shape[1:]
    assert kv_local == 1 and heads == 2 and lanes == LANES
    half = seq_count // 2
    near = pl.BlockSpec(memory_space=pltpu.VMEM)
    far = pl.BlockSpec(memory_space=pl.ANY)
    return pl.pallas_call(
        functools.partial(attention_kernel, own, heads),
        out_shape=(
            pltpu.VMEM((half, width), BF16),
            pltpu.VMEM((half, width), BF16),
            pltpu.VMEM((half, width), F32),
        ),
        in_specs=[far] * 11,
        out_specs=(near,) * 3,
        scratch_shapes=[
            pltpu.VMEM((seq_count, width), BF16),
            pltpu.VMEM((1, width), F32),
            pltpu.VMEM(query_weight.shape, BF16),
            pltpu.VMEM((lanes, width), BF16),
            pltpu.VMEM((heads, width), BF16),
            pltpu.VMEM((seq_count, cache_len, lanes), BF16),
            pltpu.VMEM(log_gates.shape, F32),
            pltpu.VMEM(out_weight.shape, BF16),
            pltpu.SMEM((seq_count,), jnp.int32),
            pltpu.SMEM((heads,), F32),
            pltpu.SemaphoreType.DMA((10,)),
            pltpu.SemaphoreType.DMA((seq_count,)),
        ],
        compiler_params=pltpu.CompilerParams(vmem_limit_bytes=ATTENTION_VMEM),
        name="attention",
    )(
        *in_hbm(
            lengths, forget_bias, tokens, norm1_gain.reshape(1, width), query_weight, key_weight.T, value_weight.T, forget_weight.T,
            kv_cache.reshape(seq_count, cache_len, lanes), log_gates, out_weight,
        ),
    )


def load_kernel(count, units, after_ref, *refs):
    del after_ref
    sources, targets, sems = refs[:count], refs[count:-1], refs[-1]
    pairs = list(zip(sources[:3], targets[:3]))
    if count > 3:
        start = pl.multiple_of(lax.axis_index("tp") * units, units)
        here = pl.ds(start, units)
        pairs += [
            (sources[3].at[:, here], targets[3].at[:, pl.ds(0, units)]),
            (sources[4].at[:, here], targets[3].at[:, pl.ds(units, units)]),
            (sources[5].at[here, :], targets[4]),
        ]
    copies = [pltpu.make_async_copy(src, dst, sems.at[i]) for i, (src, dst) in enumerate(pairs)]
    for copy in copies:
        copy.start()
    for copy in copies:
        copy.wait()


def load_weights(after, expert_weights, dense_weights, units):
    width = dense_weights[0].shape[0]
    near = pl.BlockSpec(memory_space=pltpu.VMEM)
    far = pl.BlockSpec(memory_space=pltpu.HBM)
    shapes = [weight.shape for weight in expert_weights]
    sources = list(expert_weights)
    split = units % LANES == 0
    if split:
        shapes += [(width, 2 * units), (units, width)]
        sources += dense_weights
    count = len(sources)
    loaded = pl.pallas_call(
        functools.partial(load_kernel, count, units),
        out_shape=tuple(pltpu.VMEM(shape, BF16) for shape in shapes),
        in_specs=[near] + [far] * count,
        out_specs=(near,) * len(shapes),
        scratch_shapes=[pltpu.SemaphoreType.DMA((count,))],
        compiler_params=pltpu.CompilerParams(vmem_limit_bytes=LOAD_VMEM),
        cost_estimate=pl.CostEstimate(flops=LOAD_COST, bytes_accessed=8 * width * width, transcendentals=0),
        name="load",
    )(after, *in_hbm(*sources))
    if split:
        return list(loaded)
    gate, up, down = dense_weights
    fill = -gate.shape[1] % LANES
    both = jnp.concatenate([jnp.pad(gate, ((0, 0), (0, fill))), jnp.pad(up, ((0, 0), (0, fill)))], axis=1)
    return [*loaded, both, jnp.pad(down, ((0, fill), (0, 0)))]


def ffn_kernel(
    experts, part, rows_ref, gate_ref, up_ref, down_ref, both_ref, dense_down_ref, *out_refs
):
    local, width = gate_ref.shape[:2]
    units = dense_down_ref.shape[0]
    half = rows_ref.shape[0] // 2
    first = lax.axis_index("ep") * local

    def products(at):
        values = rows_ref[at, :width]
        side = rows_ref[at, width:].astype(F32)
        lane = lax.broadcasted_iota(jnp.int32, side.shape, 1)

        def pick(column):
            hit = (lane == column) | (lane == column + experts + 1)
            return jnp.sum(jnp.where(hit, side, 0.0), axis=1, keepdims=True)

        both = jnp.dot(values, both_ref[...], preferred_element_type=F32)
        act = pick(experts) * clamped_unit(both[:, :units], both[:, units:])
        if part != units:
            unit = lax.broadcasted_iota(jnp.int32, act.shape, 1)
            start = lax.axis_index("tp") * part
            act = jnp.where((unit >= start) & (unit < start + part), act, 0.0)
        acts = [act.astype(BF16)]
        for j in range(local):
            gate_pre = jnp.dot(values, gate_ref[j], preferred_element_type=F32)
            up_pre = jnp.dot(values, up_ref[j], preferred_element_type=F32)
            acts.append((pick(first + j) * clamped_unit(gate_pre, up_pre)).astype(BF16))
        step = min(width, COLUMN_BLOCK)
        for column in range(0, width, step):
            cols = slice(column, column + step)
            mixed = jnp.dot(acts[0], dense_down_ref[:, cols], preferred_element_type=F32)
            for j in range(local):
                mixed = mixed + jnp.dot(acts[1 + j], down_ref[j, :, cols], preferred_element_type=F32)
            yield cols, mixed

    quarter = half // 2
    if 2 * half <= ROW_BLOCK:
        for cols, mixed in products(slice(0, 2 * half)):
            for i, ref in enumerate(out_refs):
                ref[:, cols] = mixed[i * quarter : (i + 1) * quarter].astype(ref.dtype)
        return
    block = min(quarter, ROW_BLOCK)

    @pl.loop(0, quarter // block)
    def _(index):
        at = pl.ds(pl.multiple_of(index * block, block), block)
        for i, ref in enumerate(out_refs):
            for cols, mixed in products(pl.ds(pl.multiple_of(index * block + i * quarter, block), block)):
                ref[at, cols] = mixed.astype(ref.dtype)


def ffn(rows, weights, experts, part):
    total = rows.shape[0]
    width = weights[0].shape[1]
    near = pl.BlockSpec(memory_space=pltpu.VMEM)
    return pl.pallas_call(
        functools.partial(ffn_kernel, experts, part),
        out_shape=tuple(pltpu.VMEM((total // 4, width), kind) for kind in (F32, F32, BF16, BF16)),
        in_specs=[near] * 6,
        out_specs=(near,) * 4,
        compiler_params=pltpu.CompilerParams(vmem_limit_bytes=FFN_VMEM),
        name="ffn",
    )(rows, *weights)


def fold_kernel(keep_ref, received_ref, stay_ref, send_ref):
    sublane = lax.broadcasted_iota(jnp.int32, (8, keep_ref.shape[1]), 0)
    for row in range(0, keep_ref.shape[0], 16):
        first, second = [
            keep_ref[at : at + 8] + received_ref[at : at + 8].astype(F32) for at in (row, row + 8)
        ]
        at = slice(row // 2, row // 2 + 8)
        stay_ref[at] = jnp.where(sublane < 4, first, pltpu.roll(second, 4, 0)).astype(stay_ref.dtype)
        send_ref[at] = jnp.where(sublane < 4, pltpu.roll(first, 4, 0), second).astype(BF16)


def fold(keep, received, outer, own, stay_type):
    count, width = keep.shape
    if outer != 2 or own != 4 or count % 16:
        total = (keep + received.astype(F32)).reshape(-1, outer, own, width)
        parts = [total[:, t].reshape(-1, width) for t in range(outer)]
        return [parts[0].astype(stay_type)] + [p.astype(BF16) for p in parts[1:]]
    near = pl.BlockSpec(memory_space=pltpu.VMEM)
    return pl.pallas_call(
        fold_kernel,
        out_shape=(
            pltpu.VMEM((count // 2, width), stay_type),
            pltpu.VMEM((count // 2, width), BF16),
        ),
        in_specs=[near] * 2,
        out_specs=(near, near),
        compiler_params=pltpu.CompilerParams(vmem_limit_bytes=NORM_VMEM),
        name="fold",
    )(keep, received)


def norm_kernel(mix_lane, shifts, *refs):
    parts, (tokens_ref, gain_ref, dense_mix_ref, side_ref, rows_ref, residual_ref) = (
        refs[: len(shifts)],
        refs[len(shifts) :],
    )
    norm_body(mix_lane, shifts, parts, tokens_ref, gain_ref, dense_mix_ref, side_ref, rows_ref, residual_ref)


def norm_body(mix_lane, shifts, parts, tokens_ref, gain_ref, dense_mix_ref, side_ref, rows_ref, residual_ref):
    width = tokens_ref.shape[1]
    sums = {}
    for shift, part in zip(shifts, parts):
        sums[shift] = sums.get(shift, 0.0) + part[...].astype(F32)
    total = sums.pop(0)
    for shift, part in sums.items():
        total = total + pltpu.roll(part, shift, 0)
    residual = tokens_ref[...] + total.astype(BF16).astype(F32)
    residual_ref[...] = residual
    hidden = rms_scaled(residual, gain_ref[...]).astype(BF16)
    rows_ref[:, :width] = hidden
    mix = jax.nn.sigmoid(jnp.sum(hidden.astype(F32) * dense_mix_ref[...], axis=1, keepdims=True))
    high = mix.astype(BF16).astype(F32)
    side = side_ref[...]
    lane = lax.broadcasted_iota(jnp.int32, side.shape, 1)
    side = jnp.where(lane == mix_lane, high, side)
    side = jnp.where(lane == 2 * mix_lane + 1, mix - high, side)
    rows_ref[:, width:] = side.astype(BF16)


def norm_rows(parts, shifts, tokens, gain, dense_mix, side, mix_lane):
    count, width = tokens.shape
    near = pl.BlockSpec(memory_space=pltpu.VMEM)
    return pl.pallas_call(
        functools.partial(norm_kernel, mix_lane, tuple(shifts)),
        out_shape=(
            pltpu.VMEM((count, width + side.shape[1]), BF16),
            pltpu.VMEM((count, width), F32),
        ),
        in_specs=[near] * (len(parts) + 4),
        out_specs=(near, near),
        compiler_params=pltpu.CompilerParams(vmem_limit_bytes=NORM_VMEM),
        name="norm",
    )(*parts, tokens, gain.reshape(1, width), dense_mix.reshape(1, width), side)


def on_device(
    tokens,
    norm1_gain,
    query_weight,
    key_weight,
    value_weight,
    forget_weight,
    forget_bias,
    out_weight,
    kv_cache,
    log_gates,
    lengths,
    norm2_gain,
    routing,
    route_weight,
    expert_gate,
    expert_up,
    expert_down,
    dense_gate,
    dense_up,
    dense_down,
    dense_mix,
):
    seq_count, width = tokens.shape
    tp_count = lax.axis_size("tp")
    ep_count = lax.axis_size("ep")
    tp_index = lax.axis_index("tp")
    own = seq_count // tp_count
    outer = tp_count // 2
    experts = expert_gate.shape[0] * ep_count

    keep, sent, tokens_near = attention(
        tokens, norm1_gain, query_weight, key_weight, value_weight, forget_weight, forget_bias,
        out_weight, kv_cache, log_gates, lengths, own,
    )

    def grouped(values):
        ordered = relative_order(values.reshape((tp_count, own) + values.shape[1:]), tp_index, tp_count)
        return ordered.reshape((outer, 2, own) + values.shape[1:])

    chosen = routing[:, :, None] == jnp.arange(experts, dtype=jnp.int32)[None, None, :]
    weights = jnp.sum(jnp.where(chosen, route_weight[:, :, None], 0.0), axis=1)
    weights = grouped(weights)[:, 0].reshape(outer * own, experts)
    parts, shifts = [keep], [0]
    for k in range(1, tp_count):
        part = swap_with(sent if k & 1 else keep, "tp", k)
        turn = k >> 1
        if outer == 2:
            shifts.append(turn * own)
        else:
            blocks = part.reshape(outer, own, width)
            part = jnp.stack([blocks[j ^ turn] for j in range(outer)]).reshape(part.shape)
            shifts.append(0)
        parts.append(part)
    high = lax.reduce_precision(weights, 8, 7)
    none = jnp.zeros((outer * own, 1), F32)
    side = jnp.concatenate([high, none, weights - high, none], axis=1)
    side = jnp.pad(side, ((0, 0), (0, -side.shape[1] % LANES)))
    rows, residual = norm_rows(
        parts, shifts, tokens_near, norm2_gain, dense_mix, side, experts
    )
    units = dense_gate.shape[1] // tp_count
    weights_near = load_weights(
        rows, [expert_gate, expert_up, expert_down], [dense_gate, dense_up, dense_down], units
    )

    stages = stages_of(ep_count)
    for offsets in stages[:0:-1]:
        others = []
        for k in offsets:
            others.append(swap_with(rows, "ep", k))
        rows = jnp.concatenate([rows] + others, axis=0)
    rows, *weights_near = lax.optimization_barrier((rows, *weights_near))

    near_other = swap_with(rows, "tp", 1)
    far = swap_with(rows, "ep", 1)
    rows = jnp.concatenate([rows, far, near_other, swap_with(far, "tp", 1)], axis=0)
    keep_near, keep_far, sent_near, sent_far = ffn(rows, weights_near, experts, units)
    received_far = swap_with(sent_far, "tp", 1)
    received_near = swap_with(sent_near, "tp", 1)
    parts = [None, fold(keep_far, received_far, outer, own, BF16)]
    parts[0] = fold(keep_near, received_near, outer, own, F32)
    mixed = parts[0][0]
    pieces = []
    for e in range(2):
        for t in range(outer):
            if e or t:
                pieces.append(swap_both(parts[e][t], e, 2 * t))
    mixed = (mixed + sum(p.astype(F32) for p in pieces)).reshape(ep_count // 2, own, width)
    for offsets in stages[1:]:
        mixed = mixed.reshape((len(offsets) + 1, -1) + mixed.shape[1:])
        pieces = []
        for i, k in enumerate(offsets):
            pieces.append(swap_with(mixed[i + 1].astype(BF16), "ep", k))
        mixed = mixed[0] + sum(p.astype(F32) for p in pieces)
    return (residual[:own] + mixed[0]).astype(BF16)


def solution(mesh):
    return jax.shard_map(
        on_device,
        mesh=mesh,
        in_specs=(
            P("ep", None),
            P(),
            P(None, "tp"),
            P(None, "tp"),
            P(None, "tp"),
            P(None, "tp"),
            P("tp"),
            P("tp", None),
            P("ep", None, "tp", None),
            P("ep", "tp", None),
            P("ep"),
            P(),
            P("ep", None),
            P("ep", None),
            P("ep", None, "tp"),
            P("ep", None, "tp"),
            P("ep", "tp", None),
            P(None, "ep"),
            P(None, "ep"),
            P("ep", None),
            P(),
        ),
        out_specs=P(("ep", "tp"), None),
        check_vma=False,
    )
```

```python
import functools

import jax
import jax.numpy as jnp
from jax import lax
from jax.experimental import pallas as pl
from jax.experimental.pallas import tpu as pltpu
from jax.sharding import PartitionSpec as P


EPS = 1e-05
LIMIT = 7.0
ALPHA = 1.702
LANES = 128
ROW_BLOCK = 128
COLUMN_BLOCK = 512
FFN_VMEM = 4 * 1024 * 1024
ATTENTION_VMEM = 16 * 1024 * 1024
LOAD_VMEM = 1024 * 1024
SEQ_BLOCK = 8
NORM_VMEM = 2 * 1024 * 1024
LOAD_COST = 4 * 10**9
BF16 = jnp.bfloat16
F32 = jnp.float32


def clamped_unit(gate_pre, up_pre):
    capped = jnp.minimum(gate_pre, LIMIT)
    return capped * jax.nn.sigmoid(ALPHA * capped) * (jnp.clip(up_pre, -LIMIT, LIMIT) + 1.0)


def rms_scaled(values, gain_vec):
    return values * lax.rsqrt(jnp.mean(values * values, axis=-1, keepdims=True) + EPS) * gain_vec


def swap_with(values, axis, offset):
    count = lax.axis_size(axis)
    return lax.ppermute(values, axis, [(i, i ^ offset) for i in range(count)])


def swap_both(values, ep_offset, tp_offset):
    ep_count, tp_count = lax.axis_size("ep"), lax.axis_size("tp")
    pairs = [
        (e * tp_count + t, (e ^ ep_offset) * tp_count + (t ^ tp_offset))
        for e in range(ep_count)
        for t in range(tp_count)
    ]
    return lax.ppermute(values, ("ep", "tp"), pairs)


def stages_of(count):
    groups = []
    bit = 1
    if bit < count:
        groups.append([bit])
        bit *= 2
    while bit < count:
        if 2 * bit < count:
            groups.append([bit, 2 * bit, 3 * bit])
            bit *= 4
        else:
            groups.append([bit])
            bit *= 2
    return groups


def relative_order(values, index, count):
    bit = 1
    while bit < count:
        pairs = values.reshape((count // (2 * bit), 2, bit) + values.shape[1:])
        swapped = jnp.where((index & bit) != 0, pairs[:, ::-1], pairs)
        values = swapped.reshape(values.shape)
        bit *= 2
    return values


def attention_kernel(
    own, heads, lengths_hbm, bias_hbm, tokens_hbm, gain_hbm, query_hbm, key_hbm, value_hbm, forget_hbm,
    cache_hbm, gates_hbm, out_hbm, keep_ref, send_ref, near_ref,
    tokens_buf, gain_buf, query_buf, pair_buf, forget_buf, cache_buf, gates_buf, out_buf,
    lengths_ref, bias_ref, sems, cache_sems,
):
    seq_count, _ = tokens_buf.shape
    cache_len, lanes = cache_buf.shape[1:]
    head_dim = lanes // 2
    rows = seq_count * heads
    tp_count = seq_count // own
    outer = tp_count // 2
    pairs = [
        (tokens_hbm, tokens_buf),
        (gain_hbm, gain_buf),
        (query_hbm, query_buf),
        (key_hbm, pair_buf.at[pl.ds(0, head_dim), :]),
        (value_hbm, pair_buf.at[pl.ds(head_dim, head_dim), :]),
        (forget_hbm, forget_buf),
        (gates_hbm, gates_buf),
        (lengths_hbm, lengths_ref),
        (bias_hbm, bias_ref),
        (out_hbm, out_buf),
    ]
    copies = [pltpu.make_async_copy(src, dst, sems.at[i]) for i, (src, dst) in enumerate(pairs)]
    cache_copies = [
        pltpu.make_async_copy(cache_hbm.at[s], cache_buf.at[s], cache_sems.at[s]) for s in range(seq_count)
    ]
    for copy in copies[:-1]:
        copy.start()

    def one_hot(condition):
        return jnp.where(condition, 1.0, 0.0).astype(BF16)

    copies[0].wait()
    copies[1].wait()
    for copy in cache_copies:
        copy.start()
    copies[-1].start()
    tokens = tokens_buf[...].astype(F32)
    normed = rms_scaled(tokens, gain_buf[...]).astype(BF16)
    spread = one_hot(
        lax.broadcasted_iota(jnp.int32, (rows, seq_count), 0) // heads
        == lax.broadcasted_iota(jnp.int32, (rows, seq_count), 1)
    )
    normed = jnp.dot(spread, normed, preferred_element_type=F32).astype(BF16)
    order = one_hot(
        chosen_rows(seq_count, seq_count, own, outer)
        == lax.broadcasted_iota(jnp.int32, (seq_count, seq_count), 1)
    )
    near_ref[...] = jnp.dot(order, tokens_buf[...], preferred_element_type=F32)[: seq_count // 2]

    transposed = (((1,), (1,)), ((), ()))
    for copy in copies[2:9]:
        copy.wait()
    queries = jnp.dot(normed, query_buf[...], preferred_element_type=F32).astype(BF16).astype(F32)
    own_pair = lax.dot_general(normed, pair_buf[...], transposed, preferred_element_type=F32)
    own_pair = own_pair.astype(BF16).astype(F32)
    forget = lax.dot_general(normed, forget_buf[...], transposed, preferred_element_type=F32)

    lane = lax.broadcasted_iota(jnp.int32, (rows, lanes), 1)
    head = lax.rem(lax.broadcasted_iota(jnp.int32, (rows, lanes), 0), heads)
    queries = jnp.where(head == 0, queries, pltpu.roll(queries, head_dim, 1))
    queries = jnp.where(lane < head_dim, queries, 0.0)
    own_score = jnp.sum(queries * own_pair, axis=1, keepdims=True)
    queries = queries.astype(BF16)

    column = lax.broadcasted_iota(jnp.int32, (rows, heads), 1)
    forget_head = lax.rem(lax.broadcasted_iota(jnp.int32, (rows, heads), 0), heads)
    forget = jnp.sum(jnp.where(column == forget_head, forget, 0.0), axis=1, keepdims=True)
    head_one = lax.rem(lax.broadcasted_iota(jnp.int32, (rows, 1), 0), heads)
    forget = forget + jnp.where(head_one == 0, bias_ref[0], bias_ref[1])
    gate_new = jnp.minimum(forget, 0.0) - jnp.log(1.0 + jnp.exp(-jnp.abs(forget)))

    group = SEQ_BLOCK
    span = group * heads
    scale = head_dim ** (-0.5)
    sequence = lax.broadcasted_iota(jnp.int32, (span, 1), 0) // heads
    place = lax.broadcasted_iota(jnp.int32, (span, cache_len), 1)
    outputs = []
    for first in range(0, seq_count, group):
        at = slice(first * heads, first * heads + span)
        scores = jnp.zeros((span, cache_len), F32)
        length = jnp.zeros((span, 1), jnp.int32)
        for i in range(group):
            cache_copies[first + i].wait()
        for i in range(group):
            found = lax.dot_general(
                queries[at], cache_buf[first + i], transposed, preferred_element_type=F32
            )
            scores = jnp.where(sequence == i, found, scores)
            length = jnp.where(sequence == i, lengths_ref[first + i], length)
        gates = jnp.concatenate([gates_buf[first + i] for i in range(group)], axis=0)
        last = jnp.sum(jnp.where(place == length - 1, gates, 0.0), axis=1, keepdims=True)
        scores = scores * scale + (last - gates + gate_new[at])
        cached = jnp.where(place < length, jnp.exp(scores), 0.0)
        own_exp = jnp.exp(own_score[at] * scale)
        denominator = jnp.sum(cached, axis=1, keepdims=True) + own_exp
        probs = (cached / denominator).astype(BF16)
        probs_own = (own_exp / denominator).astype(BF16).astype(F32)
        mixed = jnp.zeros((span, lanes), F32)
        for i in range(0, group, 2):
            both = jnp.concatenate([cache_buf[first + i], cache_buf[first + i + 1]], axis=1)
            found = jnp.dot(probs, both, preferred_element_type=F32)
            mixed = jnp.where(sequence == i, found[:, :lanes], mixed)
            mixed = jnp.where(sequence == i + 1, found[:, lanes:], mixed)
        outputs.append(mixed + probs_own * own_pair[at])
    attended = jnp.concatenate(outputs, axis=0)
    attended = jnp.where(head == 0, pltpu.roll(attended, head_dim, 1), attended)
    attended = jnp.where((lane < head_dim) == (head == 0), attended, 0.0).astype(BF16)
    gather = one_hot(
        chosen_rows(seq_count, rows, own, outer)
        == lax.broadcasted_iota(jnp.int32, (seq_count, rows), 1) // heads
    )
    attended = jnp.dot(gather, attended, preferred_element_type=F32).astype(BF16)
    copies[9].wait()
    partial = jnp.dot(attended, out_buf[...], preferred_element_type=F32)
    keep_ref[...] = partial[: seq_count // 2].astype(BF16)
    send_ref[...] = partial[seq_count // 2 :].astype(BF16)


def in_hbm(*arrays):
    return [pltpu.with_memory_space_constraint(array, pltpu.HBM) for array in arrays]


def chosen_rows(seq_count, columns, own, outer):
    place = lax.broadcasted_iota(jnp.int32, (seq_count, columns), 0)
    low = place // (outer * own)
    high = lax.rem(place // own, outer)
    owner = lax.axis_index("tp") ^ (high * 2 + low)
    return owner * own + lax.rem(place, own)


def attention(
    tokens, norm1_gain, query_weight, key_weight, value_weight, forget_weight, forget_bias,
    out_weight, kv_cache, log_gates, lengths, own,
):
    seq_count, width = tokens.shape
    heads = forget_bias.shape[0]
    cache_len, kv_local, lanes = kv_cache.shape[1:]
    assert kv_local == 1 and heads == 2 and lanes == LANES
    half = seq_count // 2
    near = pl.BlockSpec(memory_space=pltpu.VMEM)
    far = pl.BlockSpec(memory_space=pl.ANY)
    return pl.pallas_call(
        functools.partial(attention_kernel, own, heads),
        out_shape=(
            pltpu.VMEM((half, width), BF16),
            pltpu.VMEM((half, width), BF16),
            pltpu.VMEM((half, width), F32),
        ),
        in_specs=[far] * 11,
        out_specs=(near,) * 3,
        scratch_shapes=[
            pltpu.VMEM((seq_count, width), BF16),
            pltpu.VMEM((1, width), F32),
            pltpu.VMEM(query_weight.shape, BF16),
            pltpu.VMEM((lanes, width), BF16),
            pltpu.VMEM((heads, width), BF16),
            pltpu.VMEM((seq_count, cache_len, lanes), BF16),
            pltpu.VMEM(log_gates.shape, F32),
            pltpu.VMEM(out_weight.shape, BF16),
            pltpu.SMEM((seq_count,), jnp.int32),
            pltpu.SMEM((heads,), F32),
            pltpu.SemaphoreType.DMA((10,)),
            pltpu.SemaphoreType.DMA((seq_count,)),
        ],
        compiler_params=pltpu.CompilerParams(vmem_limit_bytes=ATTENTION_VMEM),
        name="attention",
    )(
        *in_hbm(
            lengths, forget_bias, tokens, norm1_gain.reshape(1, width), query_weight, key_weight.T, value_weight.T, forget_weight.T,
            kv_cache.reshape(seq_count, cache_len, lanes), log_gates, out_weight,
        ),
    )


def load_kernel(count, units, after_ref, *refs):
    del after_ref
    sources, targets, sems = refs[:count], refs[count:-1], refs[-1]
    pairs = list(zip(sources[:3], targets[:3]))
    if count > 3:
        start = pl.multiple_of(lax.axis_index("tp") * units, units)
        here = pl.ds(start, units)
        pairs += [
            (sources[3].at[:, here], targets[3].at[:, pl.ds(0, units)]),
            (sources[4].at[:, here], targets[3].at[:, pl.ds(units, units)]),
            (sources[5].at[here, :], targets[4]),
        ]
    copies = [pltpu.make_async_copy(src, dst, sems.at[i]) for i, (src, dst) in enumerate(pairs)]
    for copy in copies:
        copy.start()
    for copy in copies:
        copy.wait()


def load_weights(after, expert_weights, dense_weights, units):
    width = dense_weights[0].shape[0]
    near = pl.BlockSpec(memory_space=pltpu.VMEM)
    far = pl.BlockSpec(memory_space=pltpu.HBM)
    shapes = [weight.shape for weight in expert_weights]
    sources = list(expert_weights)
    split = units % LANES == 0
    if split:
        shapes += [(width, 2 * units), (units, width)]
        sources += dense_weights
    count = len(sources)
    loaded = pl.pallas_call(
        functools.partial(load_kernel, count, units),
        out_shape=tuple(pltpu.VMEM(shape, BF16) for shape in shapes),
        in_specs=[near] + [far] * count,
        out_specs=(near,) * len(shapes),
        scratch_shapes=[pltpu.SemaphoreType.DMA((count,))],
        compiler_params=pltpu.CompilerParams(vmem_limit_bytes=LOAD_VMEM),
        cost_estimate=pl.CostEstimate(flops=LOAD_COST, bytes_accessed=8 * width * width, transcendentals=0),
        name="load",
    )(after, *in_hbm(*sources))
    if split:
        return list(loaded)
    gate, up, down = dense_weights
    fill = -gate.shape[1] % LANES
    both = jnp.concatenate([jnp.pad(gate, ((0, 0), (0, fill))), jnp.pad(up, ((0, 0), (0, fill)))], axis=1)
    return [*loaded, both, jnp.pad(down, ((0, fill), (0, 0)))]


def ffn_kernel(
    experts, part, rows_ref, gate_ref, up_ref, down_ref, both_ref, dense_down_ref, *out_refs
):
    local, width = gate_ref.shape[:2]
    units = dense_down_ref.shape[0]
    half = rows_ref.shape[0] // 2
    first = lax.axis_index("ep") * local

    def products(at):
        values = rows_ref[at, :width]
        side = rows_ref[at, width:].astype(F32)
        lane = lax.broadcasted_iota(jnp.int32, side.shape, 1)

        def pick(column):
            hit = (lane == column) | (lane == column + experts + 1)
            return jnp.sum(jnp.where(hit, side, 0.0), axis=1, keepdims=True)

        both = jnp.dot(values, both_ref[...], preferred_element_type=F32)
        act = pick(experts) * clamped_unit(both[:, :units], both[:, units:])
        if part != units:
            unit = lax.broadcasted_iota(jnp.int32, act.shape, 1)
            start = lax.axis_index("tp") * part
            act = jnp.where((unit >= start) & (unit < start + part), act, 0.0)
        acts = [act.astype(BF16)]
        for j in range(local):
            gate_pre = jnp.dot(values, gate_ref[j], preferred_element_type=F32)
            up_pre = jnp.dot(values, up_ref[j], preferred_element_type=F32)
            acts.append((pick(first + j) * clamped_unit(gate_pre, up_pre)).astype(BF16))
        step = min(width, COLUMN_BLOCK)
        for column in range(0, width, step):
            cols = slice(column, column + step)
            mixed = jnp.dot(acts[0], dense_down_ref[:, cols], preferred_element_type=F32)
            for j in range(local):
                mixed = mixed + jnp.dot(acts[1 + j], down_ref[j, :, cols], preferred_element_type=F32)
            yield cols, mixed

    quarter = half // 2
    if 2 * half <= ROW_BLOCK:
        for cols, mixed in products(slice(0, 2 * half)):
            for i, ref in enumerate(out_refs):
                ref[:, cols] = mixed[i * quarter : (i + 1) * quarter].astype(ref.dtype)
        return
    block = min(quarter, ROW_BLOCK)

    @pl.loop(0, quarter // block)
    def _(index):
        at = pl.ds(pl.multiple_of(index * block, block), block)
        for i, ref in enumerate(out_refs):
            for cols, mixed in products(pl.ds(pl.multiple_of(index * block + i * quarter, block), block)):
                ref[at, cols] = mixed.astype(ref.dtype)


def ffn(rows, weights, experts, part):
    total = rows.shape[0]
    width = weights[0].shape[1]
    near = pl.BlockSpec(memory_space=pltpu.VMEM)
    return pl.pallas_call(
        functools.partial(ffn_kernel, experts, part),
        out_shape=tuple(pltpu.VMEM((total // 4, width), kind) for kind in (F32, F32, BF16, BF16)),
        in_specs=[near] * 6,
        out_specs=(near,) * 4,
        compiler_params=pltpu.CompilerParams(vmem_limit_bytes=FFN_VMEM),
        name="ffn",
    )(rows, *weights)


def fold_kernel(keep_ref, received_ref, stay_ref, send_ref):
    sublane = lax.broadcasted_iota(jnp.int32, (8, keep_ref.shape[1]), 0)
    for row in range(0, keep_ref.shape[0], 16):
        first, second = [
            keep_ref[at : at + 8] + received_ref[at : at + 8].astype(F32) for at in (row, row + 8)
        ]
        at = slice(row // 2, row // 2 + 8)
        stay_ref[at] = jnp.where(sublane < 4, first, pltpu.roll(second, 4, 0)).astype(stay_ref.dtype)
        send_ref[at] = jnp.where(sublane < 4, pltpu.roll(first, 4, 0), second).astype(BF16)


def fold(keep, received, outer, own, stay_type):
    count, width = keep.shape
    if outer != 2 or own != 4 or count % 16:
        total = (keep + received.astype(F32)).reshape(-1, outer, own, width)
        parts = [total[:, t].reshape(-1, width) for t in range(outer)]
        return [parts[0].astype(stay_type)] + [p.astype(BF16) for p in parts[1:]]
    near = pl.BlockSpec(memory_space=pltpu.VMEM)
    return pl.pallas_call(
        fold_kernel,
        out_shape=(
            pltpu.VMEM((count // 2, width), stay_type),
            pltpu.VMEM((count // 2, width), BF16),
        ),
        in_specs=[near] * 2,
        out_specs=(near, near),
        compiler_params=pltpu.CompilerParams(vmem_limit_bytes=NORM_VMEM),
        name="fold",
    )(keep, received)


def norm_kernel(mix_lane, shifts, *refs):
    parts, (tokens_ref, gain_ref, dense_mix_ref, side_ref, rows_ref, residual_ref) = (
        refs[: len(shifts)],
        refs[len(shifts) :],
    )
    norm_body(mix_lane, shifts, parts, tokens_ref, gain_ref, dense_mix_ref, side_ref, rows_ref, residual_ref)


def norm_body(mix_lane, shifts, parts, tokens_ref, gain_ref, dense_mix_ref, side_ref, rows_ref, residual_ref):
    width = tokens_ref.shape[1]
    sums = {}
    for shift, part in zip(shifts, parts):
        sums[shift] = sums.get(shift, 0.0) + part[...].astype(F32)
    total = sums.pop(0)
    for shift, part in sums.items():
        total = total + pltpu.roll(part, shift, 0)
    residual = tokens_ref[...] + total.astype(BF16).astype(F32)
    residual_ref[...] = residual
    hidden = rms_scaled(residual, gain_ref[...]).astype(BF16)
    rows_ref[:, :width] = hidden
    mix = jax.nn.sigmoid(jnp.sum(hidden.astype(F32) * dense_mix_ref[...], axis=1, keepdims=True))
    high = mix.astype(BF16).astype(F32)
    side = side_ref[...]
    lane = lax.broadcasted_iota(jnp.int32, side.shape, 1)
    side = jnp.where(lane == mix_lane, high, side)
    side = jnp.where(lane == 2 * mix_lane + 1, mix - high, side)
    rows_ref[:, width:] = side.astype(BF16)


def norm_rows(parts, shifts, tokens, gain, dense_mix, side, mix_lane):
    count, width = tokens.shape
    near = pl.BlockSpec(memory_space=pltpu.VMEM)
    return pl.pallas_call(
        functools.partial(norm_kernel, mix_lane, tuple(shifts)),
        out_shape=(
            pltpu.VMEM((count, width + side.shape[1]), BF16),
            pltpu.VMEM((count, width), F32),
        ),
        in_specs=[near] * (len(parts) + 4),
        out_specs=(near, near),
        compiler_params=pltpu.CompilerParams(vmem_limit_bytes=NORM_VMEM),
        name="norm",
    )(*parts, tokens, gain.reshape(1, width), dense_mix.reshape(1, width), side)


def on_device(
    tokens,
    norm1_gain,
    query_weight,
    key_weight,
    value_weight,
    forget_weight,
    forget_bias,
    out_weight,
    kv_cache,
    log_gates,
    lengths,
    norm2_gain,
    routing,
    route_weight,
    expert_gate,
    expert_up,
    expert_down,
    dense_gate,
    dense_up,
    dense_down,
    dense_mix,
):
    seq_count, width = tokens.shape
    tp_count = lax.axis_size("tp")
    ep_count = lax.axis_size("ep")
    tp_index = lax.axis_index("tp")
    own = seq_count // tp_count
    outer = tp_count // 2
    experts = expert_gate.shape[0] * ep_count

    keep, sent, tokens_near = attention(
        tokens, norm1_gain, query_weight, key_weight, value_weight, forget_weight, forget_bias,
        out_weight, kv_cache, log_gates, lengths, own,
    )

    def grouped(values):
        ordered = relative_order(values.reshape((tp_count, own) + values.shape[1:]), tp_index, tp_count)
        return ordered.reshape((outer, 2, own) + values.shape[1:])

    chosen = routing[:, :, None] == jnp.arange(experts, dtype=jnp.int32)[None, None, :]
    weights = jnp.sum(jnp.where(chosen, route_weight[:, :, None], 0.0), axis=1)
    weights = grouped(weights)[:, 0].reshape(outer * own, experts)
    parts, shifts = [keep], [0]
    for k in range(1, tp_count):
        part = swap_with(sent if k & 1 else keep, "tp", k)
        turn = k >> 1
        if outer == 2:
            shifts.append(turn * own)
        else:
            blocks = part.reshape(outer, own, width)
            part = jnp.stack([blocks[j ^ turn] for j in range(outer)]).reshape(part.shape)
            shifts.append(0)
        parts.append(part)
    high = lax.reduce_precision(weights, 8, 7)
    none = jnp.zeros((outer * own, 1), F32)
    side = jnp.concatenate([high, none, weights - high, none], axis=1)
    side = jnp.pad(side, ((0, 0), (0, -side.shape[1] % LANES)))
    rows, residual = norm_rows(
        parts, shifts, tokens_near, norm2_gain, dense_mix, side, experts
    )
    units = dense_gate.shape[1] // tp_count
    weights_near = load_weights(
        rows, [expert_gate, expert_up, expert_down], [dense_gate, dense_up, dense_down], units
    )

    stages = stages_of(ep_count)
    for offsets in stages[:0:-1]:
        others = []
        for k in offsets:
            others.append(swap_with(rows, "ep", k))
        rows = jnp.concatenate([rows] + others, axis=0)
    rows, *weights_near = lax.optimization_barrier((rows, *weights_near))

    near_other = swap_with(rows, "tp", 1)
    far = swap_with(rows, "ep", 1)
    rows = jnp.concatenate([rows, far, near_other, swap_with(far, "tp", 1)], axis=0)
    keep_near, keep_far, sent_near, sent_far = ffn(rows, weights_near, experts, units)
    received_far = swap_with(sent_far, "tp", 1)
    received_near = swap_with(sent_near, "tp", 1)
    parts = [None, fold(keep_far, received_far, outer, own, BF16)]
    parts[0] = fold(keep_near, received_near, outer, own, F32)
    mixed = parts[0][0]
    pieces = []
    for e in range(2):
        for t in range(outer):
            if e or t:
                pieces.append(swap_both(parts[e][t], e, 2 * t))
    mixed = (mixed + sum(p.astype(F32) for p in pieces)).reshape(ep_count // 2, own, width)
    for offsets in stages[1:]:
        mixed = mixed.reshape((len(offsets) + 1, -1) + mixed.shape[1:])
        pieces = []
        for i, k in enumerate(offsets):
            pieces.append(swap_with(mixed[i + 1].astype(BF16), "ep", k))
        mixed = mixed[0] + sum(p.astype(F32) for p in pieces)
    return (residual[:own] + mixed[0]).astype(BF16)


def solution(mesh):
    return jax.shard_map(
        on_device,
        mesh=mesh,
        in_specs=(
            P("ep", None),
            P(),
            P(None, "tp"),
            P(None, "tp"),
            P(None, "tp"),
            P(None, "tp"),
            P("tp"),
            P("tp", None),
            P("ep", None, "tp", None),
            P("ep", "tp", None),
            P("ep"),
            P(),
            P("ep", None),
            P("ep", None),
            P("ep", None, "tp"),
            P("ep", None, "tp"),
            P("ep", "tp", None),
            P(None, "ep"),
            P(None, "ep"),
            P("ep", None),
            P(),
        ),
        out_specs=P(("ep", "tp"), None),
        check_vma=False,
    )
```
